128 devices in a mesh: ep: 32 (over z, y, core), tp: 4 (over x).
Axes of the slice: x: 4, y: 4, z: 4, core: 2. Of those that a mesh axis runs over, the one named last changes fastest.
Arguments:
- hidden_in: bfloat16 [1536, 2048], P('ep'), may hold values from -6 to 6
- carried_state: float32 [1536, 4, 128, 256], P('ep', 'tp'), may hold values from -6 to 6
- input_gain: bfloat16 [2048], replicated, may hold values from 0.099609375 to 1.8984375
- query_weight: bfloat16 [2048, 512], P(None, 'tp'), may hold values from -0.125 to 0.125
- key_weight: bfloat16 [2048, 512], P(None, 'tp'), may hold values from -0.125 to 0.125
- value_weight: bfloat16 [2048, 1024], P(None, 'tp'), may hold values from -0.125 to 0.125
- outgate_weight: bfloat16 [2048, 1024], P(None, 'tp'), may hold values from -0.125 to 0.125
- decay_weight: bfloat16 [2048, 512], P(None, 'tp'), may hold values from -0.5 to 0.5
- decay_shift: float32 [1536, 512], P('ep', 'tp'), may hold values from -0.7 to 0
- head_gain: bfloat16 [4, 256], P('tp'), may hold values from 0.099609375 to 1.8984375
- output_weight: bfloat16 [1024, 2048], P('tp'), may hold values from -0.1875 to 0.1875
- channel_gain: bfloat16 [2048], replicated, may hold values from 0.099609375 to 1.8984375
- branch_gate: bfloat16 [2048], replicated, may hold values from -0.125 to 0.125
- routes: int32 [1536, 2], P('ep'), may hold values from 0 to 31, all different within a row; in each aligned block of 48 rows (0 to 47, 48 to 95, ...) at most 5 rows name the same one
- route_weights: float32 [1536, 2], P('ep'), may hold values from 0.1 to 1
- expert_gate: bfloat16 [32, 2048, 3072], P('ep', None, 'tp'), may hold values from -0.125 to 0.125
- expert_up: bfloat16 [32, 2048, 3072], P('ep', None, 'tp'), may hold values from -0.125 to 0.125
- expert_down: bfloat16 [32, 3072, 2048], P('ep', 'tp'), may hold values from -0.109375 to 0.109375
- dense_gate: bfloat16 [2048, 4096], P('tp', 'ep'), may hold values from -0.125 to 0.125
- dense_up: bfloat16 [2048, 4096], P('tp', 'ep'), may hold values from -0.125 to 0.125
- dense_down: bfloat16 [4096, 2048], P('ep', 'tp'), may hold values from -0.09375 to 0.09375
Outputs:
- mixed: bfloat16 [1536, 2048], P('ep', 'tp')
- new_state: float32 [1536, 4, 128, 256], P('ep', 'tp')
The draws below stay inside these ranges and needn't reach their ends.
Inputs may be any that keep to these rules, and one draw needn't show every extreme that they name: `routes`: each row names 2 different experts. Among the rows of one index of ep no expert is named more than 5 times, and in every draw some expert is named exactly 5 times by the rows of some index.
All inputs are finite; a program needn't handle non-finite values.
Results may differ from the reference program's by a relative error of at most 0.02.
Values may be sent and summed in bfloat16 or wider, within the bound.
A program may use at most 128 MiB of HBM per device.

```python
import math
import jax
import jax.numpy as jnp
import numpy as np
from jax import lax

D = 2048
HEADS = 4
DK = 128
DV = 256
FF = 3072
DFF = 4096
TOPK = 2
SEQ_DEV = 48
BATCH = 1536
EXPERTS = 32
CAP = 5
N_EP = 32
N_TP = 4


def level_of(stream_key, dims, pieces, smallest, largest):
    gain = 1.0
    for axis_at, blocks in pieces:
        draws = jax.random.uniform(jax.random.fold_in(jax.random.fold_in(stream_key, 6), axis_at), (blocks,), jnp.float32, smallest / len(pieces), largest / len(pieces))
        gain = gain * jnp.repeat(jnp.exp(draws), dims[axis_at] // blocks).reshape((-1,) + (1,) * (len(dims) - 1 - axis_at))
    return gain


def shared_out(key, own, number, rows, amount, top, limit, skew):
    ranking = jax.random.permutation(key, amount)
    crowded, common = shares(amount, rows * top, limit, skew, True), shares(amount, rows * top, limit, skew, False)
    places = jnp.arange(amount)

    def named(tallies, offset_by):
        used = int((tallies > 0).sum())
        fixed = max(1, used // 4)
        passed = fixed + (places - fixed + offset_by * (used - fixed)) % max(1, amount - fixed)
        return jnp.zeros((amount,), jnp.int32).at[ranking[jnp.where(places < fixed, places, passed)]].set(jnp.asarray(tallies, jnp.int32))

    tallies = jnp.where(number % 4 == 0, named(crowded, number // 4), named(common, number - number // 4 - 1))
    mixed = jax.random.permutation(jax.random.fold_in(own, 3), amount)
    donor, taker = mixed[0:amount // 2 * 2:2], mixed[1:amount // 2 * 2:2]
    slack = jnp.minimum(tallies[donor] - 1, limit - tallies[taker]) // 2
    slack = jnp.where((donor == ranking[0]) | (taker == ranking[0]) | (tallies[taker] == 0), 0, jnp.maximum(slack, 0))
    passed = jax.random.randint(jax.random.fold_in(own, 4), (amount // 2,), 0, 1 << 20) % (slack + 1)
    tallies = tallies.at[donor].add(-passed).at[taker].add(passed)
    members = jnp.searchsorted(jnp.cumsum(tallies), jnp.arange(rows * top), side="right").astype(jnp.int32)
    table = members.reshape(top, rows).T
    table = table[jax.random.permutation(jax.random.fold_in(own, 1), rows)]
    offset_by = jax.random.randint(jax.random.fold_in(own, 2), (rows, 1), 0, top)
    return jnp.take_along_axis(table, (jnp.arange(top)[None, :] + offset_by) % top, axis=1)


def shares(count, total, reach, slope, full):
    loads = [(1 << 20) // math.isqrt(standing ** slope) + 1 for standing in range(1, count + 1)]
    largest = reach if full else min(reach, max(-(-total // count), total * loads[0] // sum(loads)))
    least = 1 if total - largest >= count - 1 else 0
    counts, spare = [largest] + [least] * (count - 1), total - largest - least * (count - 1)
    while spare > 0:
        movable = [i for i in range(1, count) if counts[i] < largest] or [i for i in range(1, count) if counts[i] < reach]
        pool, remaining = sum([loads[i] for i in movable]), spare
        for i in movable:
            extra = min(reach - counts[i], max(1, remaining * loads[i] // pool), spare)
            counts[i] = counts[i] + extra
            spare = spare - extra
    return np.array(counts)


def gaussian(rng, dims, deviation, most, shards=(), held_as=jnp.bfloat16):
    values = deviation * jax.random.normal(rng, dims, jnp.float32)
    if shards:
        values = values * level_of(rng, dims, shards, -0.22, 0.18)
    return jnp.clip(values, -most, most).astype(held_as)


def setup_inputs(seed: int = 0) -> dict:
    streams_of = jax.random.split(jax.random.key(seed), 22)
    hidden_in = gaussian(streams_of[0], (BATCH, D), 1.0, 6.0, ((0, 32),))
    carried_state = gaussian(streams_of[1], (BATCH, HEADS, DK, DV), 1.0, 6.0, ((0, 32), (1, 4)), jnp.float32)
    input_gain = jnp.clip(1.0 + 0.18 * jax.random.normal(streams_of[2], (D,), jnp.float32), 0.099609375, 1.8984375).astype(jnp.bfloat16)
    query_weight = gaussian(streams_of[3], (D, HEADS * DK), D ** -0.5, 0.125, ((1, 4),))
    key_weight = gaussian(streams_of[4], (D, HEADS * DK), D ** -0.5, 0.125, ((1, 4),))
    value_weight = gaussian(streams_of[5], (D, HEADS * DV), D ** -0.5, 0.125, ((1, 4),))
    outgate_weight = gaussian(streams_of[6], (D, HEADS * DV), D ** -0.5, 0.125, ((1, 4),))
    decay_weight = gaussian(streams_of[7], (D, HEADS * DK), (D // 16) ** -0.5, 0.5, ((1, 4),))
    decay_shift = jnp.clip(-0.7 + 0.7 * jax.random.uniform(streams_of[8], (BATCH, HEADS * DK), jnp.float32) ** level_of(streams_of[8], (BATCH, HEADS * DK), ((0, 32), (1, 4)), -0.2, 0.2), -0.7, 0.0)
    head_gain = jnp.clip(1.0 + 0.18 * jax.random.normal(streams_of[9], (HEADS, DV), jnp.float32), 0.099609375, 1.8984375).astype(jnp.bfloat16)
    output_weight = gaussian(streams_of[10], (HEADS * DV, D), (HEADS * DV) ** -0.5, 0.1875, ((0, 4),))
    channel_gain = jnp.clip(1.0 + 0.18 * jax.random.normal(streams_of[11], (D,), jnp.float32), 0.099609375, 1.8984375).astype(jnp.bfloat16)
    branch_gate = gaussian(streams_of[12], (D,), D ** -0.5, 0.125)
    routes_keys = jax.random.split(jax.random.fold_in(streams_of[13], 1), BATCH // SEQ_DEV)
    routes_turns = jax.random.permutation(jax.random.fold_in(streams_of[13], 3), BATCH // SEQ_DEV)
    routes = jax.vmap(lambda own, number: shared_out(jax.random.fold_in(streams_of[13], 2), own, number, SEQ_DEV, EXPERTS, TOPK, CAP, 2))(routes_keys, routes_turns).reshape((BATCH, TOPK))
    route_weights = jnp.clip(0.1 + 0.9 * jax.random.uniform(streams_of[14], (BATCH, TOPK), jnp.float32) ** level_of(streams_of[14], (BATCH, TOPK), ((0, 32),), -0.2, 0.2), 0.1, 1.0)
    expert_gate = gaussian(streams_of[15], (EXPERTS, D, FF), D ** -0.5, 0.125, ((0, 32), (2, 4)))
    expert_up = gaussian(streams_of[16], (EXPERTS, D, FF), D ** -0.5, 0.125, ((0, 32), (2, 4)))
    expert_down = gaussian(streams_of[17], (EXPERTS, FF, D), FF ** -0.5, 0.109375, ((0, 32), (1, 4)))
    dense_gate = gaussian(streams_of[18], (D, DFF), D ** -0.5, 0.125, ((0, 4), (1, 32)))
    dense_up = gaussian(streams_of[19], (D, DFF), D ** -0.5, 0.125, ((0, 4), (1, 32)))
    dense_down = gaussian(streams_of[20], (DFF, D), DFF ** -0.5, 0.09375, ((0, 32), (1, 4)))
    return dict(hidden_in=hidden_in, carried_state=carried_state, input_gain=input_gain, query_weight=query_weight, key_weight=key_weight, value_weight=value_weight, outgate_weight=outgate_weight, decay_weight=decay_weight, decay_shift=decay_shift, head_gain=head_gain, output_weight=output_weight, channel_gain=channel_gain, branch_gate=branch_gate, routes=routes, route_weights=route_weights, expert_gate=expert_gate, expert_up=expert_up, expert_down=expert_down, dense_gate=dense_gate, dense_up=dense_up, dense_down=dense_down)


EPSILON = 1e-06
TAU_DECAY = 16.0

def rms_factor(values):
    return lax.rsqrt(lax.optimization_barrier(jnp.mean(values * values, axis=-1, keepdims=True)) + EPSILON)

def rounded(values):
    return lax.optimization_barrier(values.astype(jnp.bfloat16)).astype(jnp.float32)

def matmul(left, right):
    return jnp.dot(left, right, preferred_element_type=jnp.float32)

def expert_apply(token_rows, gate_matrix, up_matrix, down_matrix):
    block_width = gate_matrix.shape[1] // N_TP
    total = jnp.zeros((token_rows.shape[0], down_matrix.shape[1]), jnp.float32)
    for block in range(N_TP):
        lower = block * block_width
        gate_part = matmul(token_rows, gate_matrix[:, lower:lower + block_width])
        up_part = matmul(token_rows, up_matrix[:, lower:lower + block_width])
        hidden = (jax.nn.silu(gate_part) * up_part).astype(jnp.bfloat16)
        total = total + rounded(matmul(hidden, down_matrix[lower:lower + block_width]))
    return total

def reference(hidden_in, carried_state, input_gain, query_weight, key_weight, value_weight, outgate_weight, decay_weight, decay_shift, head_gain, output_weight, channel_gain, branch_gate, routes, route_weights, expert_gate, expert_up, expert_down, dense_gate, dense_up, dense_down):
    batch_size, width = hidden_in.shape
    head_count, key_dim, value_dim = carried_state.shape[1:]
    inputs = hidden_in.astype(jnp.float32)
    normed = (inputs * rms_factor(inputs) * input_gain.astype(jnp.float32)).astype(jnp.bfloat16)
    query = matmul(normed, query_weight).astype(jnp.bfloat16)
    key_rows = matmul(normed, key_weight).astype(jnp.bfloat16)
    value_rows = matmul(normed, value_weight).astype(jnp.bfloat16)
    outgate = matmul(normed, outgate_weight).astype(jnp.bfloat16)
    decay = jnp.exp(jax.nn.log_sigmoid(matmul(normed, decay_weight)) / TAU_DECAY + decay_shift)
    decay = decay.reshape(batch_size, head_count, key_dim)
    query_scaled = query.astype(jnp.float32).reshape(batch_size, head_count, key_dim) * key_dim ** (-0.5)
    key_vals = key_rows.astype(jnp.float32).reshape(batch_size, head_count, key_dim)
    value_vals = value_rows.astype(jnp.float32).reshape(batch_size, head_count, value_dim)
    new_state = decay[..., None] * carried_state + key_vals[..., None] * value_vals[:, :, None, :]
    readout = jnp.einsum('bhk,bhkv->bhv', query_scaled, new_state, precision=lax.Precision.HIGHEST)
    gate_vals = jax.nn.silu(outgate.astype(jnp.float32).reshape(batch_size, head_count, value_dim))
    gated = (readout * rms_factor(readout) * head_gain.astype(jnp.float32) * gate_vals).astype(jnp.bfloat16)
    group = head_count // N_TP
    attended = jnp.zeros((batch_size, width), jnp.float32)
    for block in range(N_TP):
        head_rows = gated[:, block * group:(block + 1) * group].reshape(batch_size, group * value_dim)
        weight_rows = output_weight[block * group * value_dim:(block + 1) * group * value_dim]
        attended = attended + rounded(matmul(head_rows, weight_rows))
    middle = rounded(inputs + attended)
    scaled = middle * rms_factor(middle) * channel_gain.astype(jnp.float32)
    branch = jax.nn.sigmoid(lax.optimization_barrier(jnp.sum(scaled * branch_gate.astype(jnp.float32), axis=-1)))
    ffn_in = scaled.astype(jnp.bfloat16)
    dense_hidden = (jax.nn.silu(matmul(ffn_in, dense_gate)) * matmul(ffn_in, dense_up)).astype(jnp.bfloat16)
    dense = matmul(dense_hidden, dense_down)
    topk = routes.shape[1]
    flat_routes = routes.reshape(-1)
    flat_tokens = (jnp.arange(flat_routes.shape[0], dtype=jnp.int32) // topk).astype(jnp.int32)
    flat_weights = route_weights.reshape(-1)
    capacity = N_EP * CAP

    def one_expert(carry, index):
        order = jnp.argsort((flat_routes != index).astype(jnp.int32), stable=True)[:capacity]
        valid = flat_routes[order] == index
        token_ids = flat_tokens[order]
        result = expert_apply(ffn_in[token_ids], expert_gate[index], expert_up[index], expert_down[index])
        weights = jnp.where(valid, flat_weights[order], jnp.zeros_like(flat_weights[order]))
        return (carry.at[token_ids].add(weights[:, None] * result), None)
    routed, _ = lax.scan(one_expert, jnp.zeros((batch_size, width), jnp.float32), jnp.arange(expert_gate.shape[0], dtype=jnp.int32))
    mixed = (middle + branch[:, None] * dense + routed).astype(jnp.bfloat16)
    return (mixed, new_state)
```

```python
import functools

import jax
import jax.numpy as jnp
from jax import lax
from jax.experimental import pallas as pl
from jax.experimental.pallas import tpu as pltpu
from jax.sharding import PartitionSpec as P

EPSILON = 1e-06
TAU_DECAY = 16.0
MESH = pl.DeviceIdType.MESH
CAP = 5
ROWS = 6
PAD = 8
Z_SIZE = 4
F32 = jnp.float32
BF16 = jnp.bfloat16


def dot(left, right):
    return jnp.dot(left, right, preferred_element_type=F32)


def rms_factor(values):
    return lax.rsqrt(jnp.mean(values * values, axis=-1, keepdims=True) + EPSILON)


def silu(values):
    return values * jax.nn.sigmoid(values)


def attention_kernel(
    experts,
    hid_ref,
    gain_ref,
    shift_ref,
    hgain_ref,
    routes_ref,
    rw_ref,
    qw_hbm,
    kw_hbm,
    vw_hbm,
    ow_hbm,
    dw_hbm,
    pw_hbm,
    state_hbm,
    part_ref,
    state_out,
    sel_ref,
    comb_hi_ref,
    comb_lo_ref,
    qw,
    kw,
    vw,
    ow,
    dw,
    pw,
    st,
    q_s,
    k_s,
    v_s,
    d_s,
    ro_s,
    w_sem,
    in_sem,
    out_sem,
):
    tokens, key_dim = q_s.shape
    groups = tokens // 8
    pairs = ((dw_hbm, dw), (qw_hbm, qw), (kw_hbm, kw), (vw_hbm, vw))
    w_copies = [pltpu.make_async_copy(s, d, w_sem.at[i]) for i, (s, d) in enumerate(pairs)]
    for copy in w_copies:
        copy.start()

    def state_in(g):
        rows = pl.ds(g * 8, 8)
        return pltpu.make_async_copy(state_hbm.at[rows], st.at[rows], in_sem.at[g])

    def state_back(g):
        rows = pl.ds(g * 8, 8)
        return pltpu.make_async_copy(st.at[rows], state_out.at[rows], out_sem.at[g])

    for g in range(groups):
        state_in(g).start()
    o_copy = pltpu.make_async_copy(ow_hbm, ow, w_sem.at[4])
    o_copy.start()
    p_copy = pltpu.make_async_copy(pw_hbm, pw, w_sem.at[5])
    p_copy.start()

    slots = experts * PAD
    e_at = lax.broadcasted_iota(jnp.int32, (tokens, experts), 1)
    r0, r1 = routes_ref[:, 0:1], routes_ref[:, 1:2]
    oh0, oh1 = (e_at == r0).astype(F32), (e_at == r1).astype(F32)
    tri = (
        lax.broadcasted_iota(jnp.int32, (tokens, tokens), 0)
        > lax.broadcasted_iota(jnp.int32, (tokens, tokens), 1)
    ).astype(F32)
    before0 = dot(tri, oh0)
    before1 = dot(tri, oh1) + jnp.sum(oh0, axis=0, keepdims=True)
    slot0 = jnp.sum(before0 * oh0, axis=1, keepdims=True)
    slot1 = jnp.sum(before1 * oh1, axis=1, keepdims=True)
    pos0 = r0 * PAD + slot0.astype(jnp.int32)
    pos1 = r1 * PAD + slot1.astype(jnp.int32)
    at = lax.broadcasted_iota(jnp.int32, (tokens, slots), 1)
    hit0, hit1 = (at == pos0).astype(F32), (at == pos1).astype(F32)
    sel_ref[...] = (hit0 + hit1).astype(BF16)
    comb = hit0 * rw_ref[:, 0:1] + hit1 * rw_ref[:, 1:2]
    comb_hi = comb.astype(BF16)
    comb_hi_ref[...] = comb_hi
    comb_lo_ref[...] = (comb - comb_hi.astype(F32)).astype(BF16)

    hid = hid_ref[...].astype(F32)
    normed = (hid * rms_factor(hid) * gain_ref[...].astype(F32)).astype(BF16)
    w_copies[0].wait()
    pre = dot(normed, dw[...])
    log_sig = jnp.minimum(pre, 0.0) - jnp.log1p(jnp.exp(-jnp.abs(pre)))
    d_s[...] = jnp.exp(log_sig / TAU_DECAY + shift_ref[...])
    w_copies[1].wait()
    q_s[...] = dot(normed, qw[...]).astype(BF16).astype(F32) * key_dim ** (-0.5)
    w_copies[2].wait()
    k_s[...] = dot(normed, kw[...]).astype(BF16).astype(F32)
    w_copies[3].wait()
    v_s[...] = dot(normed, vw[...]).astype(BF16).astype(F32)

    def group(g, carry):
        state_in(g).wait()
        rows = pl.ds(pl.multiple_of(g * 8, 8), 8)
        d_t, k_t, q_t = d_s[rows, :].T, k_s[rows, :].T, q_s[rows, :].T
        v_8 = v_s[rows, :]
        outs = []
        for j in range(8):
            new = d_t[:, j : j + 1] * st[g * 8 + j] + k_t[:, j : j + 1] * v_8[j : j + 1, :]
            st[g * 8 + j] = new
            outs.append(jnp.sum(q_t[:, j : j + 1] * new, axis=0, keepdims=True))
        ro_s[rows, :] = jnp.concatenate(outs, axis=0)

        @pl.when(g > 0)
        def _():
            state_back(g - 1).start()

        return carry

    lax.fori_loop(0, groups, group, 0)

    o_copy.wait()
    outgate = dot(normed, ow[...]).astype(BF16).astype(F32)
    readout = ro_s[...]
    gated = readout * rms_factor(readout) * hgain_ref[...].astype(F32) * silu(outgate)
    state_back(groups - 1).start()
    p_copy.wait()
    part_ref[...] = dot(gated.astype(BF16), pw[...]).astype(BF16)
    for g in range(groups):
        state_back(g).wait()


def attention(experts, hid, gain, shift, hgain, routes, rw, weights, pw, state):
    tokens, width = hid.shape
    key_dim, value_dim = state.shape[1:]
    slots = experts * PAD
    vmem = pl.BlockSpec(memory_space=pltpu.VMEM)
    anyspace = pl.BlockSpec(memory_space=pltpu.HBM)
    groups = tokens // 8
    return pl.pallas_call(
        functools.partial(attention_kernel, experts),
        name="attention",
        out_shape=(
            jax.ShapeDtypeStruct((tokens, width), BF16),
            jax.ShapeDtypeStruct(state.shape, F32),
            jax.ShapeDtypeStruct((tokens, slots), BF16),
            jax.ShapeDtypeStruct((tokens, slots), BF16),
            jax.ShapeDtypeStruct((tokens, slots), BF16),
        ),
        in_specs=[vmem] * 6 + [anyspace] * 7,
        out_specs=(vmem, anyspace, vmem, vmem, vmem),
        scratch_shapes=[pltpu.VMEM(w.shape, BF16) for w in weights]
        + [
            pltpu.VMEM(pw.shape, BF16),
            pltpu.VMEM(state.shape, F32),
            pltpu.VMEM((tokens, key_dim), F32),
            pltpu.VMEM((tokens, key_dim), F32),
            pltpu.VMEM((tokens, value_dim), F32),
            pltpu.VMEM((tokens, key_dim), F32),
            pltpu.VMEM((tokens, value_dim), F32),
            pltpu.SemaphoreType.DMA((6,)),
            pltpu.SemaphoreType.DMA((groups,)),
            pltpu.SemaphoreType.DMA((groups,)),
        ],
        compiler_params=pltpu.CompilerParams(vmem_limit_bytes=40 << 20),
    )(hid, gain, shift, hgain, routes, rw, *weights, pw, state)


def branches_kernel(
    sizes,
    part_ref,
    hid_ref,
    gain_ref,
    bgate_ref,
    sel_ref,
    comb_hi_ref,
    comb_lo_ref,
    eg_hbm,
    eu_hbm,
    ed_hbm,
    dg_hbm,
    du_hbm,
    dd_hbm,
    out_ref,
    eg,
    eu,
    ed,
    wgu,
    wd,
    rs1,
    mid,
    snd,
    rcv,
    ffn_all,
    pr,
    rs2,
    hid_all,
    db,
    dr,
    hbuf,
    yb,
    yr,
    rb,
    ret,
    local_sem,
    wz_send,
    wz_recv,
    x_send,
    x_recv,
    yc_send,
    yc_recv,
    pl_send,
    pl_recv,
):
    n_ep, n_x, n_z = sizes
    n_yc = n_ep // n_z
    tokens, width = hid_ref.shape
    quarter = width // n_x
    units = dg_hbm.shape[1]
    all_units = n_z * units
    ep, x = lax.axis_index("ep"), lax.axis_index("tp")
    z, yc = ep // n_yc, ep % n_yc

    def x_peer(i):
        return (ep, lax.rem(x + i, n_x))

    def z_peer(i):
        return (lax.rem(z + i, n_z) * n_yc + yc, x)

    def yc_peer(i):
        return (z * n_yc + lax.rem(yc + i, n_yc), x)

    def ep_peer(i):
        return (lax.rem(ep + i, n_ep), x)

    def remote(src, dst, send, recv, device):
        return pltpu.make_async_remote_copy(
            src_ref=src,
            dst_ref=dst,
            send_sem=send,
            recv_sem=recv,
            device_id=device,
            device_id_type=MESH,
        )

    e_copies = [
        pltpu.make_async_copy(s, d, local_sem.at[i])
        for i, (s, d) in enumerate(((eg_hbm, eg), (eu_hbm, eu), (ed_hbm, ed)))
    ]

    def unit_block(offset):
        return pl.ds(pl.multiple_of(offset + z * units, units), units)

    places = (
        (dg_hbm, wgu.at[:, unit_block(0)]),
        (du_hbm, wgu.at[:, unit_block(all_units)]),
        (dd_hbm, wd.at[unit_block(0), :]),
    )
    d_copies = [
        pltpu.make_async_copy(s, d, local_sem.at[3 + i]) for i, (s, d) in enumerate(places)
    ]

    rcv[...] = jnp.zeros_like(rcv)
    ret[...] = jnp.zeros_like(ret)

    barrier = pltpu.get_barrier_semaphore()
    for i in range(1, n_x):
        pl.semaphore_signal(barrier, inc=1, device_id=x_peer(i), device_id_type=MESH)

    def greet(i, carry):
        pl.semaphore_signal(barrier, inc=1, device_id=ep_peer(i), device_id_type=MESH)
        return carry

    lax.fori_loop(1, n_ep, greet, 0)
    for copy in d_copies + e_copies:
        copy.start()
    pl.semaphore_wait(barrier, n_x - 1 + n_ep - 1)

    def lanes(i):
        return pl.ds(pl.multiple_of(lax.rem(x + i, n_x) * quarter, quarter), quarter)

    rs1_copies = [
        remote(part_ref.at[:, lanes(i)], rs1.at[i], x_send.at[0, i], x_recv.at[0, i], x_peer(i))
        for i in range(1, n_x)
    ]
    for copy in rs1_copies:
        copy.start()
    wz_copies = [
        remote(s, d, wz_send.at[i, k], wz_recv.at[i, k], z_peer(i))
        for i in range(1, n_z)
        for k, (s, d) in enumerate(places)
    ]
    for copy in wz_copies:
        copy.start()
    total = part_ref[:, lanes(0)].astype(F32)
    for i, copy in zip(range(1, n_x), rs1_copies):
        copy.wait_recv()
        total = total + rs1[i].astype(F32)
    middle_q = (hid_ref[:, lanes(0)].astype(F32) + total).astype(BF16)
    mid[pl.ds(x, 1)] = middle_q[None]

    mid_copies = [
        remote(mid.at[x], mid.at[x], x_send.at[1, i], x_recv.at[1, i], x_peer(i))
        for i in range(1, n_x)
    ]
    for copy in mid_copies:
        copy.start()
    for copy in mid_copies:
        copy.wait_recv()
    squares = sum(
        jnp.sum(mid[i].astype(F32) * mid[i].astype(F32), axis=-1, keepdims=True) for i in range(n_x)
    )
    factor = lax.rsqrt(squares / width + EPSILON)
    own_scaled = mid[pl.ds(x, 1)][0].astype(F32) * factor * gain_ref[:, lanes(0)].astype(F32)
    ffn_all[pl.ds(yc, 1)] = own_scaled.astype(BF16)[None]
    yc_copies = [
        remote(
            ffn_all.at[yc], ffn_all.at[yc], yc_send.at[0, i], yc_recv.at[0, i], yc_peer(i)
        )
        for i in range(1, n_yc)
    ]
    for copy in yc_copies:
        copy.start()
    logit = jnp.zeros((tokens, 1), F32)
    for i in range(n_x):
        part = slice(i * quarter, (i + 1) * quarter)
        scaled = mid[i].astype(F32) * factor * gain_ref[:, part].astype(F32)
        logit = logit + jnp.sum(scaled * bgate_ref[:, part].astype(F32), axis=-1, keepdims=True)
        rows = lax.dot_general(
            sel_ref[...], scaled.astype(BF16), (((0,), (0,)), ((), ())), preferred_element_type=F32
        )
        snd[:, :, part] = rows.reshape(n_ep, PAD, quarter).astype(BF16)
    branch = jax.nn.sigmoid(logit)

    def dispatch(i, carry):
        to = lax.rem(ep + i, n_ep)
        remote(
            snd.at[to, pl.ds(0, ROWS)],
            rcv.at[ep, pl.ds(0, ROWS)],
            pl_send.at[0],
            pl_recv.at[0],
            (to, x),
        ).start()
        return carry

    lax.fori_loop(1, n_ep, dispatch, 0)
    rcv[pl.ds(ep, 1)] = snd[pl.ds(ep, 1)]

    for copy in d_copies:
        copy.wait()
    for copy in wz_copies:
        copy.wait_recv()
    for copy in yc_copies:
        copy.wait_recv()
    per_x = n_yc // n_x

    def paired_of(i):
        mine = ffn_all[pl.ds(lax.rem(x + i, n_x) * per_x, per_x)]
        return dot(mine.reshape(per_x * tokens, quarter), wgu[...])

    rs2_copies = []
    for i in range(1, n_x):
        pr[i] = paired_of(i).astype(BF16)
        rs2_copies.append(
            remote(pr.at[i], rs2.at[i], x_send.at[2, i], x_recv.at[2, i], x_peer(i))
        )
        rs2_copies[-1].start()
    paired = paired_of(0)

    for copy in e_copies:
        copy.wait()
    arrived = rcv.at[pl.ds(0, n_ep - 1), pl.ds(0, ROWS)]
    pltpu.make_async_copy(arrived, arrived, pl_recv.at[0]).wait()
    flat = n_ep * PAD
    tile = 256

    def hidden_tile(j, carry):
        cols = pl.ds(pl.multiple_of(j * tile, tile), tile)
        rows = rcv[...].reshape(flat, width)
        gate, up = dot(rows, eg[:, cols]), dot(rows, eu[:, cols])
        hbuf[:, cols] = (silu(gate) * up).astype(BF16)
        return carry

    lax.fori_loop(0, eg.shape[1] // tile, hidden_tile, 0)

    def expert_out(i):
        return dot(hbuf[...], ed[:, lanes(i)]).reshape(n_ep, PAD, quarter)

    y_copies = []
    for i in range(1, n_x):
        yb[i] = expert_out(i).astype(BF16)
        y_copies.append(
            remote(
                yb.at[i, :, pl.ds(0, ROWS)],
                yr.at[i, :, pl.ds(0, ROWS)],
                x_send.at[3, i],
                x_recv.at[3, i],
                x_peer(i),
            )
        )
        y_copies[-1].start()
    own_out = expert_out(0).astype(BF16).astype(F32)

    for i, copy in zip(range(1, n_x), rs2_copies):
        copy.wait_recv()
        paired = paired + rs2[i].astype(F32)
    hidden = (silu(paired[:, :all_units]) * paired[:, all_units:]).astype(BF16)
    block = pl.ds(x * per_x, per_x)
    hid_all[block] = hidden.reshape(per_x, tokens, all_units)
    h_copies = [
        remote(
            hid_all.at[block], hid_all.at[block], x_send.at[4, i], x_recv.at[4, i], x_peer(i)
        )
        for i in range(1, n_x)
    ]
    for copy in h_copies:
        copy.start()

    for i, copy in zip(range(1, n_x), y_copies):
        copy.wait_recv()
        own_out = own_out + yr[i].astype(F32)
    rb[...] = own_out.astype(BF16)

    def send_home(i, carry):
        to = lax.rem(ep + i, n_ep)
        remote(
            rb.at[to, pl.ds(0, ROWS)],
            ret.at[ep, pl.ds(0, ROWS)],
            pl_send.at[1],
            pl_recv.at[1],
            (to, x),
        ).start()
        return carry

    lax.fori_loop(1, n_ep, send_home, 0)
    ret[pl.ds(ep, 1)] = rb[pl.ds(ep, 1)]

    for copy in h_copies:
        copy.wait_recv()
    dense_part = dot(hid_all[...].reshape(n_yc * tokens, all_units), wd[...])
    db[...] = dense_part.reshape(n_yc, tokens, quarter).astype(BF16)
    db_copies = [
        remote(
            db.at[lax.rem(yc + i, n_yc)],
            dr.at[i],
            yc_send.at[1, i],
            yc_recv.at[1, i],
            yc_peer(i),
        )
        for i in range(1, n_yc)
    ]
    for copy in db_copies:
        copy.start()

    dense = db[pl.ds(yc, 1)][0].astype(F32)
    for i, copy in zip(range(1, n_yc), db_copies):
        copy.wait_recv()
        dense = dense + dr[i].astype(F32)
    home = ret.at[pl.ds(0, n_ep - 1), pl.ds(0, ROWS)]
    pltpu.make_async_copy(home, home, pl_recv.at[1]).wait()
    back = ret[...].reshape(flat, quarter)
    routed = dot(comb_hi_ref[...], back) + dot(comb_lo_ref[...], back)
    middle_own = mid[pl.ds(x, 1)][0].astype(F32)
    out_ref[...] = (middle_own + branch * dense + routed).astype(BF16)

    for copy in rs1_copies + mid_copies + rs2_copies + y_copies + h_copies:
        copy.wait_send()
    for copy in wz_copies + yc_copies + db_copies:
        copy.wait_send()
    sent = snd.at[pl.ds(0, n_ep - 1), pl.ds(0, ROWS)]
    pltpu.make_async_copy(sent, sent, pl_send.at[0]).wait()
    sent_home = rb.at[pl.ds(0, n_ep - 1), pl.ds(0, ROWS)]
    pltpu.make_async_copy(sent_home, sent_home, pl_send.at[1]).wait()


def branches(sizes, part, hid, gain, bgate, sel, comb_hi, comb_lo, eg, eu, ed, dg, du, dd):
    n_ep, n_x, n_z = sizes
    n_yc = n_ep // n_z
    tokens, width = hid.shape
    quarter, units = width // n_x, dg.shape[1]
    all_units = n_z * units
    flat = n_ep * PAD
    group_rows = n_yc * tokens // n_x
    vmem = pl.BlockSpec(memory_space=pltpu.VMEM)
    anyspace = pl.BlockSpec(memory_space=pltpu.HBM)
    dma = pltpu.SemaphoreType.DMA
    return pl.pallas_call(
        functools.partial(branches_kernel, sizes),
        name="branches",
        out_shape=jax.ShapeDtypeStruct((tokens, quarter), BF16),
        in_specs=[vmem] * 7 + [anyspace] * 6,
        out_specs=vmem,
        scratch_shapes=[
            pltpu.VMEM(eg.shape, BF16),
            pltpu.VMEM(eu.shape, BF16),
            pltpu.VMEM(ed.shape, BF16),
            pltpu.VMEM((quarter, 2 * all_units), BF16),
            pltpu.VMEM((all_units, quarter), BF16),
            pltpu.VMEM((n_x, tokens, quarter), BF16),
            pltpu.VMEM((n_x, tokens, quarter), BF16),
            pltpu.VMEM((n_ep, PAD, width), BF16),
            pltpu.VMEM((n_ep, PAD, width), BF16),
            pltpu.VMEM((n_yc, tokens, quarter), BF16),
            pltpu.VMEM((n_x, group_rows, 2 * all_units), BF16),
            pltpu.VMEM((n_x, group_rows, 2 * all_units), BF16),
            pltpu.VMEM((n_yc, tokens, all_units), BF16),
            pltpu.VMEM((n_yc, tokens, quarter), BF16),
            pltpu.VMEM((n_yc, tokens, quarter), BF16),
            pltpu.VMEM((flat, eg.shape[1]), BF16),
            pltpu.VMEM((n_x, n_ep, PAD, quarter), BF16),
            pltpu.VMEM((n_x, n_ep, PAD, quarter), BF16),
            pltpu.VMEM((n_ep, PAD, quarter), BF16),
            pltpu.VMEM((n_ep, PAD, quarter), BF16),
            dma((6,)),
            dma((n_z, 3)),
            dma((n_z, 3)),
            dma((5, n_x)),
            dma((5, n_x)),
            dma((2, n_yc)),
            dma((2, n_yc)),
            dma((2,)),
            dma((2,)),
        ],
        compiler_params=pltpu.CompilerParams(
            collective_id=0, has_side_effects=True, vmem_limit_bytes=48 << 20
        ),
    )(part, hid, gain, bgate, sel, comb_hi, comb_lo, eg, eu, ed, dg, du, dd)


def body(
    sizes,
    hidden_in,
    carried_state,
    input_gain,
    query_weight,
    key_weight,
    value_weight,
    outgate_weight,
    decay_weight,
    decay_shift,
    head_gain,
    output_weight,
    channel_gain,
    branch_gate,
    routes,
    route_weights,
    expert_gate,
    expert_up,
    expert_down,
    dense_gate,
    dense_up,
    dense_down,
):
    width = hidden_in.shape[1]
    part, new_state, sel, comb_hi, comb_lo = attention(
        sizes[0],
        hidden_in,
        input_gain.reshape(1, width),
        decay_shift,
        head_gain,
        routes,
        route_weights,
        (query_weight, key_weight, value_weight, outgate_weight, decay_weight),
        output_weight,
        carried_state[:, 0],
    )
    mixed = branches(
        sizes,
        part,
        hidden_in,
        channel_gain.reshape(1, width),
        branch_gate.reshape(1, width),
        sel,
        comb_hi,
        comb_lo,
        expert_gate[0],
        expert_up[0],
        expert_down[0],
        dense_gate,
        dense_up,
        dense_down,
    )
    return (mixed, new_state[:, None])


def solution(mesh):
    in_specs = (
        P("ep", None),
        P("ep", "tp", None, None),
        P(),
        P(None, "tp"),
        P(None, "tp"),
        P(None, "tp"),
        P(None, "tp"),
        P(None, "tp"),
        P("ep", "tp"),
        P("tp", None),
        P("tp", None),
        P(),
        P(),
        P("ep", None),
        P("ep", None),
        P("ep", None, "tp"),
        P("ep", None, "tp"),
        P("ep", "tp", None),
        P("tp", "ep"),
        P("tp", "ep"),
        P("ep", "tp"),
    )
    out_specs = (P("ep", "tp"), P("ep", "tp", None, None))
    n_ep = mesh.shape["ep"]
    sizes = (n_ep, mesh.shape["tp"], min(Z_SIZE, n_ep // 2))
    return jax.shard_map(
        functools.partial(body, sizes),
        mesh=mesh,
        in_specs=in_specs,
        out_specs=out_specs,
        check_vma=False,
    )
```

```python
import functools

import jax
import jax.numpy as jnp
from jax import lax
from jax.experimental import pallas as pl
from jax.experimental.pallas import tpu as pltpu
from jax.sharding import PartitionSpec as P

EPSILON = 1e-06
TAU_DECAY = 16.0
MESH = pl.DeviceIdType.MESH
CAP = 5
ROWS = 6
VMEM_ALL = 67043328
PAD = 8
Z_SIZE = 4
F32 = jnp.float32
BF16 = jnp.bfloat16


def dot(left, right):
    return jnp.dot(left, right, preferred_element_type=F32)


def in_hbm(*arrays):
    return [pltpu.with_memory_space_constraint(a, pltpu.HBM) for a in arrays]


def turned_dot(left, right):
    return lax.dot_general(left, right, (((0,), (0,)), ((), ())), preferred_element_type=F32)


def rms_factor(values):
    return lax.rsqrt(jnp.mean(values * values, axis=-1, keepdims=True) + EPSILON)


def silu(values):
    return values * jax.nn.sigmoid(values)


def attention_kernel(
    experts,
    routes_hbm,
    rw_hbm,
    hid_hbm,
    gain_hbm,
    shift_hbm,
    hgain_hbm,
    qw_hbm,
    kw_hbm,
    vw_hbm,
    ow_hbm,
    dw_hbm,
    pw_hbm,
    state_hbm,
    part_ref,
    state_out,
    sel_ref,
    comb_hi_ref,
    comb_lo_ref,
    routes_s,
    rw_s,
    hid_s,
    gain_s,
    shift_s,
    hgain_s,
    qw,
    kw,
    vw,
    ow,
    dw,
    pw,
    st,
    q_s,
    k_s,
    v_s,
    d_s,
    ro_s,
    w_sem,
    in_sem,
    out_sem,
):
    tokens, key_dim = q_s.shape
    groups = tokens // 8
    small = (
        (routes_hbm, routes_s),
        (rw_hbm, rw_s),
        (hid_hbm, hid_s),
        (gain_hbm, gain_s),
        (shift_hbm, shift_s),
        (hgain_hbm, hgain_s),
    )
    s_copies = [pltpu.make_async_copy(s, d, w_sem.at[6 + i]) for i, (s, d) in enumerate(small)]
    for copy in s_copies:
        copy.start()
    pairs = ((dw_hbm, dw), (qw_hbm, qw), (kw_hbm, kw), (vw_hbm, vw))
    w_copies = [pltpu.make_async_copy(s, d, w_sem.at[i]) for i, (s, d) in enumerate(pairs)]
    for copy in w_copies:
        copy.start()

    def state_in(g):
        rows = pl.ds(g * 8, 8)
        return pltpu.make_async_copy(state_hbm.at[rows], st.at[rows], in_sem.at[g])

    def state_back(g):
        rows = pl.ds(g * 8, 8)
        return pltpu.make_async_copy(st.at[rows], state_out.at[rows], out_sem.at[g])

    for g in range(groups):
        state_in(g).start()
    o_copy = pltpu.make_async_copy(ow_hbm, ow, w_sem.at[4])
    o_copy.start()
    p_copy = pltpu.make_async_copy(pw_hbm, pw, w_sem.at[5])
    p_copy.start()

    for copy in s_copies[:2]:
        copy.wait()
    slots = experts * PAD
    e_at = lax.broadcasted_iota(jnp.int32, (experts, tokens), 0)
    r0, r1 = routes_s[0:1, :], routes_s[1:2, :]
    oh0, oh1 = (e_at == r0).astype(F32), (e_at == r1).astype(F32)
    tri = (
        lax.broadcasted_iota(jnp.int32, (tokens, tokens), 0)
        < lax.broadcasted_iota(jnp.int32, (tokens, tokens), 1)
    ).astype(F32)
    before0 = dot(oh0, tri)
    before1 = dot(oh1, tri) + jnp.sum(oh0, axis=1, keepdims=True)
    slot0 = jnp.sum(before0 * oh0, axis=0, keepdims=True)
    slot1 = jnp.sum(before1 * oh1, axis=0, keepdims=True)
    pos0 = r0 * PAD + slot0.astype(jnp.int32)
    pos1 = r1 * PAD + slot1.astype(jnp.int32)
    at = lax.broadcasted_iota(jnp.int32, (slots, tokens), 0)
    hit0, hit1 = (at == pos0).astype(F32), (at == pos1).astype(F32)
    sel_ref[...] = (hit0 + hit1).astype(BF16)
    comb = hit0 * rw_s[0:1, :] + hit1 * rw_s[1:2, :]
    comb_hi = comb.astype(BF16)
    comb_hi_ref[...] = comb_hi
    comb_lo_ref[...] = (comb - comb_hi.astype(F32)).astype(BF16)

    for copy in s_copies[2:]:
        copy.wait()
    hid = hid_s[...].astype(F32)
    normed = (hid * rms_factor(hid) * gain_s[...][None, :].astype(F32)).astype(BF16)
    w_copies[0].wait()
    pre = dot(normed, dw[...])
    log_sig = jnp.minimum(pre, 0.0) - jnp.log1p(jnp.exp(-jnp.abs(pre)))
    d_s[...] = jnp.exp(log_sig / TAU_DECAY + shift_s[...])
    w_copies[1].wait()
    q_s[...] = dot(normed, qw[...]).astype(BF16).astype(F32) * key_dim ** (-0.5)
    w_copies[2].wait()
    k_s[...] = dot(normed, kw[...]).astype(BF16).astype(F32)
    w_copies[3].wait()
    v_s[...] = dot(normed, vw[...]).astype(BF16).astype(F32)

    def group(g, carry):
        state_in(g).wait()
        rows = pl.ds(pl.multiple_of(g * 8, 8), 8)
        d_t, k_t, q_t = d_s[rows, :].T, k_s[rows, :].T, q_s[rows, :].T
        v_8 = v_s[rows, :]
        outs = []
        for j in range(8):
            new = d_t[:, j : j + 1] * st[g * 8 + j] + k_t[:, j : j + 1] * v_8[j : j + 1, :]
            st[g * 8 + j] = new
            outs.append(jnp.sum(q_t[:, j : j + 1] * new, axis=0, keepdims=True))
        ro_s[rows, :] = jnp.concatenate(outs, axis=0)

        @pl.when(g > 0)
        def _():
            state_back(g - 1).start()

        return carry

    lax.fori_loop(0, groups, group, 0)

    o_copy.wait()
    outgate = dot(normed, ow[...]).astype(BF16).astype(F32)
    readout = ro_s[...]
    gated = readout * rms_factor(readout) * hgain_s[...].astype(F32) * silu(outgate)
    state_back(groups - 1).start()
    p_copy.wait()
    part_ref[...] = dot(gated.astype(BF16), pw[...]).astype(BF16)
    for g in range(groups):
        state_back(g).wait()


def attention(experts, hid, gain, shift, hgain, routes, rw, weights, pw, state):
    tokens, width = hid.shape
    key_dim, value_dim = state.shape[1:]
    slots = experts * PAD
    vmem = pl.BlockSpec(memory_space=pltpu.VMEM)
    anyspace = pl.BlockSpec(memory_space=pltpu.HBM)
    groups = tokens // 8
    return pl.pallas_call(
        functools.partial(attention_kernel, experts),
        name="attention",
        out_shape=(
            jax.ShapeDtypeStruct((tokens, width), BF16),
            jax.ShapeDtypeStruct(state.shape, F32),
            jax.ShapeDtypeStruct((slots, tokens), BF16),
            jax.ShapeDtypeStruct((slots, tokens), BF16),
            jax.ShapeDtypeStruct((slots, tokens), BF16),
        ),
        in_specs=[anyspace] * 13,
        out_specs=(vmem, anyspace, vmem, vmem, vmem),
        scratch_shapes=[
            pltpu.VMEM(a.shape, a.dtype)
            for a in (routes, rw, hid, gain, shift, hgain) + tuple(weights)
        ]
        + [
            pltpu.VMEM(pw.shape, BF16),
            pltpu.VMEM(state.shape, F32),
            pltpu.VMEM((tokens, key_dim), F32),
            pltpu.VMEM((tokens, key_dim), F32),
            pltpu.VMEM((tokens, value_dim), F32),
            pltpu.VMEM((tokens, key_dim), F32),
            pltpu.VMEM((tokens, value_dim), F32),
            pltpu.SemaphoreType.DMA((12,)),
            pltpu.SemaphoreType.DMA((groups,)),
            pltpu.SemaphoreType.DMA((groups,)),
        ],
        compiler_params=pltpu.CompilerParams(vmem_limit_bytes=40 << 20),
    )(*in_hbm(routes, rw, hid, gain, shift, hgain, *weights, pw, state))


def branches_kernel(
    sizes,
    part_ref,
    hid_ref,
    gain_ref,
    bgate_ref,
    sel_ref,
    comb_hi_ref,
    comb_lo_ref,
    eg_hbm,
    eu_hbm,
    ed_hbm,
    dg_hbm,
    du_hbm,
    dd_hbm,
    out_ref,
    eg,
    eu,
    ed,
    wgu,
    wd,
    rs1,
    mid,
    snd,
    rcv,
    ffn_all,
    pr,
    rs2,
    hid_all,
    db,
    dr,
    hbuf,
    yb,
    yr,
    rb,
    ret,
    local_sem,
    wz_send,
    wz_recv,
    x_send,
    x_recv,
    yc_send,
    yc_recv,
    pl_send,
    pl_recv,
):
    n_ep, n_x, n_z = sizes
    n_yc = n_ep // n_z
    tokens, width = hid_ref.shape
    quarter = width // n_x
    units = dg_hbm.shape[1]
    all_units = n_z * units
    ep, x = lax.axis_index("ep"), lax.axis_index("tp")
    z, yc = ep // n_yc, ep % n_yc

    def x_peer(i):
        return (ep, lax.rem(x + i, n_x))

    def z_peer(i):
        return (lax.rem(z + i, n_z) * n_yc + yc, x)

    def yc_peer(i):
        return (z * n_yc + lax.rem(yc + i, n_yc), x)

    def ep_peer(i):
        return (lax.rem(ep + i, n_ep), x)

    def remote(src, dst, send, recv, device):
        return pltpu.make_async_remote_copy(
            src_ref=src,
            dst_ref=dst,
            send_sem=send,
            recv_sem=recv,
            device_id=device,
            device_id_type=MESH,
        )

    e_copies = [
        pltpu.make_async_copy(s, d, local_sem.at[i])
        for i, (s, d) in enumerate(((eg_hbm, eg), (eu_hbm, eu), (ed_hbm, ed)))
    ]

    def unit_block(offset):
        return pl.ds(pl.multiple_of(offset + z * units, units), units)

    places = (
        (dg_hbm, wgu.at[:, unit_block(0)]),
        (du_hbm, wgu.at[:, unit_block(all_units)]),
        (dd_hbm, wd.at[unit_block(0), :]),
    )
    d_copies = [
        pltpu.make_async_copy(s, d, local_sem.at[3 + i]) for i, (s, d) in enumerate(places)
    ]

    rcv[...] = jnp.zeros_like(rcv)
    ret[...] = jnp.zeros_like(ret)

    barrier = pltpu.get_barrier_semaphore()
    for i in range(1, n_x):
        pl.semaphore_signal(barrier, inc=1, device_id=x_peer(i), device_id_type=MESH)

    def greet(i, carry):
        pl.semaphore_signal(barrier, inc=1, device_id=ep_peer(i), device_id_type=MESH)
        return carry

    lax.fori_loop(1, n_ep, greet, 0)
    for copy in d_copies + e_copies:
        copy.start()
    pl.semaphore_wait(barrier, n_x - 1 + n_ep - 1)

    def lanes(i):
        return pl.ds(pl.multiple_of(lax.rem(x + i, n_x) * quarter, quarter), quarter)

    rs1_copies = [
        remote(part_ref.at[:, lanes(i)], rs1.at[i], x_send.at[0, i], x_recv.at[0, i], x_peer(i))
        for i in range(1, n_x)
    ]
    for copy in rs1_copies:
        copy.start()
    wz_copies = [
        remote(s, d, wz_send.at[i, k], wz_recv.at[i, k], z_peer(i))
        for i in range(1, n_z)
        for k, (s, d) in enumerate(places)
    ]
    for copy in wz_copies:
        copy.start()
    total = part_ref[:, lanes(0)].astype(F32)
    for i, copy in zip(range(1, n_x), rs1_copies):
        copy.wait_recv()
        total = total + rs1[i].astype(F32)
    middle_q = (hid_ref[:, lanes(0)].astype(F32) + total).astype(BF16)
    mid[pl.ds(x, 1)] = middle_q[None]

    mid_copies = [
        remote(mid.at[x], mid.at[x], x_send.at[1, i], x_recv.at[1, i], x_peer(i))
        for i in range(1, n_x)
    ]
    for copy in mid_copies:
        copy.start()
    for copy in mid_copies:
        copy.wait_recv()
    squares = sum(
        jnp.sum(mid[i].astype(F32) * mid[i].astype(F32), axis=-1, keepdims=True) for i in range(n_x)
    )
    factor = lax.rsqrt(squares / width + EPSILON)
    own_scaled = mid[pl.ds(x, 1)][0].astype(F32) * factor * gain_ref[lanes(0)][None, :].astype(F32)
    ffn_all[pl.ds(yc, 1)] = own_scaled.astype(BF16)[None]
    yc_copies = [
        remote(
            ffn_all.at[yc], ffn_all.at[yc], yc_send.at[0, i], yc_recv.at[0, i], yc_peer(i)
        )
        for i in range(1, n_yc)
    ]
    for copy in yc_copies:
        copy.start()
    logit = jnp.zeros((tokens, 1), F32)
    for i in range(n_x):
        part = slice(i * quarter, (i + 1) * quarter)
        scaled = mid[i].astype(F32) * factor * gain_ref[part][None, :].astype(F32)
        logit = logit + jnp.sum(scaled * bgate_ref[part][None, :].astype(F32), axis=-1, keepdims=True)
        rows = dot(sel_ref[...], scaled.astype(BF16))
        snd[:, :, part] = rows.reshape(n_ep, PAD, quarter).astype(BF16)
    branch = jax.nn.sigmoid(logit)

    def dispatch(i, carry):
        to = lax.rem(ep + i, n_ep)
        remote(
            snd.at[to, pl.ds(0, ROWS)],
            rcv.at[ep, pl.ds(0, ROWS)],
            pl_send.at[0],
            pl_recv.at[0],
            (to, x),
        ).start()
        return carry

    lax.fori_loop(1, n_ep, dispatch, 0)
    rcv[pl.ds(ep, 1)] = snd[pl.ds(ep, 1)]

    for copy in d_copies:
        copy.wait()
    for copy in wz_copies:
        copy.wait_recv()
    for copy in yc_copies:
        copy.wait_recv()
    per_x = n_yc // n_x

    def paired_of(i):
        mine = ffn_all[pl.ds(lax.rem(x + i, n_x) * per_x, per_x)]
        return dot(mine.reshape(per_x * tokens, quarter), wgu[...])

    rs2_copies = []
    for i in range(1, n_x):
        pr[i] = paired_of(i).astype(BF16)
        rs2_copies.append(
            remote(pr.at[i], rs2.at[i], x_send.at[2, i], x_recv.at[2, i], x_peer(i))
        )
        rs2_copies[-1].start()
    paired = paired_of(0)

    for copy in e_copies:
        copy.wait()
    arrived = rcv.at[pl.ds(0, n_ep - 1), pl.ds(0, ROWS)]
    pltpu.make_async_copy(arrived, arrived, pl_recv.at[0]).wait()
    flat = n_ep * PAD
    tile = 256

    def hidden_tile(j, carry):
        cols = pl.ds(pl.multiple_of(j * tile, tile), tile)
        rows = rcv[...].reshape(flat, width)
        gate, up = dot(rows, eg[:, cols]), dot(rows, eu[:, cols])
        hbuf[:, cols] = (silu(gate) * up).astype(BF16)
        return carry

    lax.fori_loop(0, eg.shape[1] // tile, hidden_tile, 0)

    def expert_out(i):
        return dot(hbuf[...], ed[:, lanes(i)]).reshape(n_ep, PAD, quarter)

    y_copies = []
    for i in range(1, n_x):
        yb[i] = expert_out(i).astype(BF16)
        y_copies.append(
            remote(
                yb.at[i, :, pl.ds(0, ROWS)],
                yr.at[i, :, pl.ds(0, ROWS)],
                x_send.at[3, i],
                x_recv.at[3, i],
                x_peer(i),
            )
        )
        y_copies[-1].start()
    own_out = expert_out(0).astype(BF16).astype(F32)

    for i, copy in zip(range(1, n_x), rs2_copies):
        copy.wait_recv()
        paired = paired + rs2[i].astype(F32)
    hidden = (silu(paired[:, :all_units]) * paired[:, all_units:]).astype(BF16)
    block = pl.ds(x * per_x, per_x)
    hid_all[block] = hidden.reshape(per_x, tokens, all_units)
    h_copies = [
        remote(
            hid_all.at[block], hid_all.at[block], x_send.at[4, i], x_recv.at[4, i], x_peer(i)
        )
        for i in range(1, n_x)
    ]
    for copy in h_copies:
        copy.start()

    for i, copy in zip(range(1, n_x), y_copies):
        copy.wait_recv()
        own_out = own_out + yr[i].astype(F32)
    rb[...] = own_out.astype(BF16)

    def send_home(i, carry):
        to = lax.rem(ep + i, n_ep)
        remote(
            rb.at[to, pl.ds(0, ROWS)],
            ret.at[ep, pl.ds(0, ROWS)],
            pl_send.at[1],
            pl_recv.at[1],
            (to, x),
        ).start()
        return carry

    lax.fori_loop(1, n_ep, send_home, 0)
    ret[pl.ds(ep, 1)] = rb[pl.ds(ep, 1)]

    for copy in h_copies:
        copy.wait_recv()
    dense_part = dot(hid_all[...].reshape(n_yc * tokens, all_units), wd[...])
    db[...] = dense_part.reshape(n_yc, tokens, quarter).astype(BF16)
    db_copies = [
        remote(
            db.at[lax.rem(yc + i, n_yc)],
            dr.at[i],
            yc_send.at[1, i],
            yc_recv.at[1, i],
            yc_peer(i),
        )
        for i in range(1, n_yc)
    ]
    for copy in db_copies:
        copy.start()

    dense = db[pl.ds(yc, 1)][0].astype(F32)
    for i, copy in zip(range(1, n_yc), db_copies):
        copy.wait_recv()
        dense = dense + dr[i].astype(F32)
    home = ret.at[pl.ds(0, n_ep - 1), pl.ds(0, ROWS)]
    pltpu.make_async_copy(home, home, pl_recv.at[1]).wait()
    back = ret[...].reshape(flat, quarter)
    routed = turned_dot(comb_hi_ref[...], back) + turned_dot(comb_lo_ref[...], back)
    middle_own = mid[pl.ds(x, 1)][0].astype(F32)
    out_ref[...] = (middle_own + branch * dense + routed).astype(BF16)

    for copy in rs1_copies + mid_copies + rs2_copies + y_copies + h_copies:
        copy.wait_send()
    for copy in wz_copies + yc_copies + db_copies:
        copy.wait_send()
    sent = snd.at[pl.ds(0, n_ep - 1), pl.ds(0, ROWS)]
    pltpu.make_async_copy(sent, sent, pl_send.at[0]).wait()
    sent_home = rb.at[pl.ds(0, n_ep - 1), pl.ds(0, ROWS)]
    pltpu.make_async_copy(sent_home, sent_home, pl_send.at[1]).wait()


def branches(sizes, part, hid, gain, bgate, sel, comb_hi, comb_lo, eg, eu, ed, dg, du, dd):
    n_ep, n_x, n_z = sizes
    n_yc = n_ep // n_z
    tokens, width = hid.shape
    quarter, units = width // n_x, dg.shape[1]
    all_units = n_z * units
    flat = n_ep * PAD
    group_rows = n_yc * tokens // n_x
    vmem = pl.BlockSpec(memory_space=pltpu.VMEM)
    anyspace = pl.BlockSpec(memory_space=pltpu.HBM)
    dma = pltpu.SemaphoreType.DMA
    return pl.pallas_call(
        functools.partial(branches_kernel, sizes),
        name="branches",
        out_shape=jax.ShapeDtypeStruct((tokens, quarter), BF16),
        in_specs=[vmem] * 7 + [anyspace] * 6,
        out_specs=vmem,
        scratch_shapes=[
            pltpu.VMEM(eg.shape, BF16),
            pltpu.VMEM(eu.shape, BF16),
            pltpu.VMEM(ed.shape, BF16),
            pltpu.VMEM((quarter, 2 * all_units), BF16),
            pltpu.VMEM((all_units, quarter), BF16),
            pltpu.VMEM((n_x, tokens, quarter), BF16),
            pltpu.VMEM((n_x, tokens, quarter), BF16),
            pltpu.VMEM((n_ep, PAD, width), BF16),
            pltpu.VMEM((n_ep, PAD, width), BF16),
            pltpu.VMEM((n_yc, tokens, quarter), BF16),
            pltpu.VMEM((n_x, group_rows, 2 * all_units), BF16),
            pltpu.VMEM((n_x, group_rows, 2 * all_units), BF16),
            pltpu.VMEM((n_yc, tokens, all_units), BF16),
            pltpu.VMEM((n_yc, tokens, quarter), BF16),
            pltpu.VMEM((n_yc, tokens, quarter), BF16),
            pltpu.VMEM((flat, eg.shape[1]), BF16),
            pltpu.VMEM((n_x, n_ep, PAD, quarter), BF16),
            pltpu.VMEM((n_x, n_ep, PAD, quarter), BF16),
            pltpu.VMEM((n_ep, PAD, quarter), BF16),
            pltpu.VMEM((n_ep, PAD, quarter), BF16),
            dma((6,)),
            dma((n_z, 3)),
            dma((n_z, 3)),
            dma((5, n_x)),
            dma((5, n_x)),
            dma((2, n_yc)),
            dma((2, n_yc)),
            dma((2,)),
            dma((2,)),
        ],
        compiler_params=pltpu.CompilerParams(
            collective_id=0, has_side_effects=True, vmem_limit_bytes=48 << 20
        ),
    )(part, hid, gain, bgate, sel, comb_hi, comb_lo, *in_hbm(eg, eu, ed, dg, du, dd))


def body(
    sizes,
    hidden_in,
    carried_state,
    input_gain,
    query_weight,
    key_weight,
    value_weight,
    outgate_weight,
    decay_weight,
    decay_shift,
    head_gain,
    output_weight,
    channel_gain,
    branch_gate,
    routes,
    route_weights,
    expert_gate,
    expert_up,
    expert_down,
    dense_gate,
    dense_up,
    dense_down,
):
    part, new_state, sel, comb_hi, comb_lo = attention(
        sizes[0],
        hidden_in,
        input_gain,
        decay_shift,
        head_gain,
        routes.T,
        route_weights.T,
        (query_weight, key_weight, value_weight, outgate_weight, decay_weight),
        output_weight,
        carried_state[:, 0],
    )
    mixed = branches(
        sizes,
        part,
        hidden_in,
        channel_gain,
        branch_gate,
        sel,
        comb_hi,
        comb_lo,
        expert_gate[0],
        expert_up[0],
        expert_down[0],
        dense_gate,
        dense_up,
        dense_down,
    )
    return (mixed, new_state[:, None])


def solution(mesh):
    in_specs = (
        P("ep", None),
        P("ep", "tp", None, None),
        P(),
        P(None, "tp"),
        P(None, "tp"),
        P(None, "tp"),
        P(None, "tp"),
        P(None, "tp"),
        P("ep", "tp"),
        P("tp", None),
        P("tp", None),
        P(),
        P(),
        P("ep", None),
        P("ep", None),
        P("ep", None, "tp"),
        P("ep", None, "tp"),
        P("ep", "tp", None),
        P("tp", "ep"),
        P("tp", "ep"),
        P("ep", "tp"),
    )
    out_specs = (P("ep", "tp"), P("ep", "tp", None, None))
    n_ep = mesh.shape["ep"]
    sizes = (n_ep, mesh.shape["tp"], min(Z_SIZE, n_ep // 2))
    return jax.shard_map(
        functools.partial(body, sizes),
        mesh=mesh,
        in_specs=in_specs,
        out_specs=out_specs,
        check_vma=False,
    )
```

```python
import functools

import jax
import jax.numpy as jnp
from jax import lax
from jax.experimental import pallas as pl
from jax.experimental.pallas import tpu as pltpu
from jax.sharding import PartitionSpec as P

EPSILON = 1e-06
TAU_DECAY = 16.0
MESH = pl.DeviceIdType.MESH
CAP = 5
ROWS = 6
VMEM_ALL = 67043328
PAD = 8
CHUNKS = 4
EARLY = 2
FLIGHT = 2
Z_SIZE = 4
F32 = jnp.float32
BF16 = jnp.bfloat16


def dot(left, right):
    return jnp.dot(left, right, preferred_element_type=F32)


def in_hbm(*arrays):
    return [pltpu.with_memory_space_constraint(a, pltpu.HBM) for a in arrays]


def turned_dot(left, right):
    return lax.dot_general(left, right, (((0,), (0,)), ((), ())), preferred_element_type=F32)


def rms_factor(values):
    return lax.rsqrt(jnp.mean(values * values, axis=-1, keepdims=True) + EPSILON)


def silu(values):
    return values * jax.nn.sigmoid(values)


def layer_kernel(
    sizes,
    routes_hbm,
    rw_hbm,
    hid_hbm,
    gain_hbm,
    shift_hbm,
    hgain_hbm,
    cgain_hbm,
    bgate_hbm,
    qw_hbm,
    kw_hbm,
    vw_hbm,
    ow_hbm,
    dw_hbm,
    pw_hbm,
    state_hbm,
    eg_hbm,
    eu_hbm,
    ed_hbm,
    dg_hbm,
    du_hbm,
    dd_hbm,
    out_ref,
    state_out,
    routes_s,
    rw_s,
    hid_s,
    gain_s,
    shift_s,
    hgain_s,
    cgain_s,
    bgate_s,
    qw,
    kw,
    vw,
    ow,
    dw,
    pw,
    q_s,
    k_s,
    v_s,
    d_s,
    ro_s,
    part,
    sel_ref,
    comb_hi_ref,
    comb_lo_ref,
    eg,
    eu,
    ed,
    wgu,
    wd,
    rs1,
    mid,
    snd,
    rcv,
    mid_all,
    ffn,
    fac,
    pr,
    rs2,
    hid_all,
    db,
    dr,
    yb,
    yr,
    rb,
    ret,
    w_sem,
    in_sem,
    local_sem,
    wz_send,
    wz_recv,
    x_send,
    x_recv,
    r_send,
    r_recv,
    y_send,
    y_recv,
    yc_send,
    yc_recv,
    pl_send,
    pl_recv,
):
    n_ep, n_x, n_z = sizes
    n_yc = n_ep // n_z
    n_y = n_yc // 2
    tokens, width = hid_s.shape
    key_dim = q_s.shape[1]
    groups = tokens // 8
    quarter = width // n_x
    units = dg_hbm.shape[1]
    all_units = n_z * units
    per_chunk = n_ep // CHUNKS
    ep, x = lax.axis_index("ep"), lax.axis_index("tp")
    z, yc = ep // n_yc, ep % n_yc
    y, c = yc // 2, yc % 2

    def x_peer(i):
        return (ep, lax.rem(x + i, n_x))

    def z_peer(i):
        return (lax.rem(z + i, n_z) * n_yc + yc, x)

    def yc_peer(i):
        return (z * n_yc + lax.rem(yc + i, n_yc), x)

    def offsets(r):
        k, j = r // per_chunk, r % per_chunk
        return j // 2, (j % 2) * 2 + k % 2, k // 2

    def ep_at(r, sign):
        dz, dy, dc = offsets(r)
        there_z = lax.rem(z + n_z + sign * dz, n_z)
        there_y = lax.rem(y + n_y + sign * dy, n_y)
        return (there_z * n_yc + there_y * 2 + lax.rem(c + dc, 2), x)

    def remote(src, dst, send, recv, device):
        return pltpu.make_async_remote_copy(
            src_ref=src,
            dst_ref=dst,
            send_sem=send,
            recv_sem=recv,
            device_id=device,
            device_id_type=MESH,
        )

    def lanes(i):
        return pl.ds(pl.multiple_of(lax.rem(x + i, n_x) * quarter, quarter), quarter)

    peers_x, peers_z, peers_yc = pl.ds(1, n_x - 1), pl.ds(1, n_z - 1), pl.ds(1, n_yc - 1)

    def wait_bytes(ref, sem):
        pltpu.make_async_copy(ref, ref, sem).wait()

    small = (
        (routes_hbm, routes_s),
        (rw_hbm, rw_s),
        (hid_hbm, hid_s),
        (gain_hbm, gain_s),
        (shift_hbm, shift_s),
        (hgain_hbm, hgain_s),
        (cgain_hbm, cgain_s),
        (bgate_hbm, bgate_s),
    )
    s_copies = [pltpu.make_async_copy(s, d, w_sem.at[6 + i]) for i, (s, d) in enumerate(small)]
    pairs = ((dw_hbm, dw), (qw_hbm, qw), (kw_hbm, kw), (vw_hbm, vw), (ow_hbm, ow), (pw_hbm, pw))
    w_copies = [pltpu.make_async_copy(s, d, w_sem.at[i]) for i, (s, d) in enumerate(pairs)]
    for copy in s_copies + w_copies[:4]:
        copy.start()

    def state_in(g):
        rows = pl.ds(g * 8, 8)
        return pltpu.make_async_copy(state_hbm.at[rows], state_out.at[rows], in_sem.at[g])

    places = ((dg_hbm, wgu.at[0, 0]), (du_hbm, wgu.at[0, 1]), (dd_hbm, wd.at[0]))
    d_copies = [
        pltpu.make_async_copy(s, d, local_sem.at[3 + i]) for i, (s, d) in enumerate(places)
    ]
    e_copies = [
        pltpu.make_async_copy(s, d, local_sem.at[i])
        for i, (s, d) in enumerate(((eg_hbm, eg), (eu_hbm, eu), (ed_hbm, ed)))
    ]

    rcv[...] = jnp.zeros_like(rcv)
    ret[...] = jnp.zeros_like(ret)
    barrier = pltpu.get_barrier_semaphore()
    for i in range(1, n_x):
        pl.semaphore_signal(barrier, inc=1, device_id=x_peer(i), device_id_type=MESH)
    for r in range(1, n_ep):
        pl.semaphore_signal(barrier, inc=1, device_id=ep_at(r, 1), device_id_type=MESH)
    for copy in d_copies:
        copy.start()
    for g in range(groups):
        state_in(g).start()
    for copy in w_copies[4:] + e_copies:
        copy.start()

    for copy in s_copies[:2]:
        copy.wait()
    slots = n_ep * PAD
    e_at = lax.broadcasted_iota(jnp.int32, (n_ep, tokens), 0)
    r0, r1 = routes_s[0:1, :], routes_s[1:2, :]
    oh0, oh1 = (e_at == r0).astype(F32), (e_at == r1).astype(F32)
    tri = (
        lax.broadcasted_iota(jnp.int32, (tokens, tokens), 0)
        < lax.broadcasted_iota(jnp.int32, (tokens, tokens), 1)
    ).astype(F32)
    before0 = dot(oh0, tri)
    before1 = dot(oh1, tri) + jnp.sum(oh0, axis=1, keepdims=True)
    slot0 = jnp.sum(before0 * oh0, axis=0, keepdims=True)
    slot1 = jnp.sum(before1 * oh1, axis=0, keepdims=True)

    def place_of(route):
        dz = ((route >> 3) - z) & 3
        dy = (((route >> 1) & 3) - y) & 3
        dc = ((route & 1) - c) & 1
        return (dc * 2 + (dy & 1)) * per_chunk + dz * 2 + (dy >> 1)

    pos0 = place_of(r0) * PAD + slot0.astype(jnp.int32)
    pos1 = place_of(r1) * PAD + slot1.astype(jnp.int32)
    at = lax.broadcasted_iota(jnp.int32, (slots, tokens), 0)
    hit0, hit1 = (at == pos0).astype(F32), (at == pos1).astype(F32)
    sel_ref[...] = (hit0 + hit1).astype(BF16)
    comb = hit0 * rw_s[0:1, :] + hit1 * rw_s[1:2, :]
    comb_hi = comb.astype(BF16)
    comb_hi_ref[...] = comb_hi
    comb_lo_ref[...] = (comb - comb_hi.astype(F32)).astype(BF16)

    for copy in d_copies:
        copy.wait()
    pl.semaphore_wait(barrier, n_x - 1 + n_ep - 1)
    near_first = [1, n_z - 1] + list(range(2, n_z - 1))
    for i in near_first:
        b = n_z - i
        remote(wgu.at[0], wgu.at[b], wz_send.at[0], wz_recv.at[b], z_peer(i)).start()

    for copy in s_copies[2:]:
        copy.wait()
    hid = hid_s[...].astype(F32)
    normed = (hid * rms_factor(hid) * gain_s[...][None, :].astype(F32)).astype(BF16)
    w_copies[0].wait()
    pre = dot(normed, dw[...])
    log_sig = jnp.minimum(pre, 0.0) - jnp.log1p(jnp.exp(-jnp.abs(pre)))
    d_s[...] = jnp.exp(log_sig / TAU_DECAY + shift_s[...])
    w_copies[1].wait()
    q_s[...] = dot(normed, qw[...]).astype(BF16).astype(F32) * key_dim ** (-0.5)
    w_copies[2].wait()
    k_s[...] = dot(normed, kw[...]).astype(BF16).astype(F32)
    w_copies[3].wait()
    v_s[...] = dot(normed, vw[...]).astype(BF16).astype(F32)

    def group(g, carry):
        state_in(g).wait()
        rows = pl.ds(pl.multiple_of(g * 8, 8), 8)
        d_t, k_t, q_t = d_s[rows, :].T, k_s[rows, :].T, q_s[rows, :].T
        v_8 = v_s[rows, :]
        outs = []
        for j in range(8):
            b = g * 8 + j
            new = d_t[:, j : j + 1] * state_out[b] + k_t[:, j : j + 1] * v_8[j : j + 1, :]
            state_out[b] = new
            outs.append(jnp.sum(q_t[:, j : j + 1] * new, axis=0, keepdims=True))
        ro_s[rows, :] = jnp.concatenate(outs, axis=0)
        return carry

    lax.fori_loop(0, groups, group, 0)

    w_copies[4].wait()
    outgate = dot(normed, ow[...]).astype(BF16).astype(F32)
    readout = ro_s[...]
    gated = readout * rms_factor(readout) * hgain_s[...].astype(F32) * silu(outgate)
    gated = gated.astype(BF16)
    w_copies[5].wait()

    for i in range(1, n_x):
        part[i] = dot(gated, pw[:, lanes(i)]).astype(BF16)
        remote(part.at[i], rs1.at[i], x_send.at[0], x_recv.at[0], x_peer(i)).start()
    total = dot(gated, pw[:, lanes(0)]).astype(BF16).astype(F32)

    wait_bytes(rs1.at[peers_x], x_recv.at[0])
    for i in range(1, n_x):
        total = total + rs1[i].astype(F32)
    middle_q = (hid_s[:, lanes(0)].astype(F32) + total).astype(BF16)
    mid[pl.ds(x, 1)] = middle_q[None]
    mid_all[pl.ds(yc, 1)] = middle_q[None]

    for i in range(1, n_x):
        remote(mid.at[x], mid.at[x], x_send.at[1], x_recv.at[1], x_peer(i)).start()
    for i in range(1, n_yc):
        remote(mid_all.at[yc], mid_all.at[yc], yc_send.at[0], yc_recv.at[0], yc_peer(i)).start()

    wait_bytes(mid.at[peers_x], x_recv.at[1])

    squares = sum(
        jnp.sum(mid[i].astype(F32) * mid[i].astype(F32), axis=-1, keepdims=True) for i in range(n_x)
    )
    factor = lax.rsqrt(squares / width + EPSILON)
    logit = jnp.zeros((tokens, 1), F32)
    for i in range(n_x):
        cols = slice(i * quarter, (i + 1) * quarter)
        scaled = mid[i].astype(F32) * factor * cgain_s[cols][None, :].astype(F32)
        logit = logit + jnp.sum(scaled * bgate_s[cols][None, :].astype(F32), axis=-1, keepdims=True)
        ffn[:, cols] = scaled.astype(BF16)
    branch = jax.nn.sigmoid(logit)

    def chunk(k):
        return pl.ds(k * per_chunk, per_chunk)

    def others(k):
        first = 1 if k == 0 else 0
        return pl.ds(k * per_chunk + first, per_chunk - first)

    def dispatch(k):
        for r in range(k * per_chunk, (k + 1) * per_chunk):
            if r:
                remote(
                    snd.at[r, pl.ds(0, ROWS)],
                    rcv.at[r, pl.ds(0, ROWS)],
                    pl_send.at[k],
                    pl_recv.at[k],
                    ep_at(r, 1),
                ).start()

    for k in range(CHUNKS):
        rows = dot(sel_ref[k * per_chunk * PAD : (k + 1) * per_chunk * PAD, :], ffn[...])
        snd[chunk(k)] = rows.reshape(per_chunk, PAD, width).astype(BF16)
        if k < FLIGHT:
            dispatch(k)
    rcv[0] = snd[0]
    factor_rows = jnp.broadcast_to(factor, (tokens, 128)).T[0:8, :]
    fac[pl.ds(yc, 1), :, 0:tokens] = factor_rows[None]
    for i in range(1, n_yc):
        remote(fac.at[yc], fac.at[yc], yc_send.at[2], yc_recv.at[2], yc_peer(i)).start()

    wait_bytes(mid_all.at[peers_yc], yc_recv.at[0])

    per_x = n_yc // n_x
    gain_q = cgain_s[lanes(0)][None, :].astype(F32)
    rows_in = mid_all[...].reshape(n_yc * tokens, quarter).astype(F32) * gain_q
    rows_in = rows_in.astype(BF16)

    def group_of(i):
        return pl.ds(lax.rem(x + i, n_x) * per_x, per_x)

    for b in [0] + near_first:
        if b:
            wait_bytes(wgu.at[b], wz_recv.at[b])
        paired = dot(rows_in, jnp.concatenate([wgu[b, 0], wgu[b, 1]], axis=1))
        pr[b] = paired.astype(BF16).reshape(n_yc, tokens, 2 * units)
        for i in range(1, n_x):
            remote(
                pr.at[b, group_of(i)], rs2.at[b, i], r_send.at[b], r_recv.at[b], x_peer(i)
            ).start()

    for copy in e_copies:
        copy.wait()
    flat = per_chunk * PAD

    def run_expert(k):
        wait_bytes(rcv.at[others(k), pl.ds(0, ROWS)], pl_recv.at[k])
        if k + FLIGHT < CHUNKS:
            dispatch(k + FLIGHT)
        rows = rcv[chunk(k)].reshape(flat, width)
        hidden = (silu(dot(rows, eg[...])) * dot(rows, eu[...])).astype(BF16)
        for i in list(range(1, n_x)) + [0]:
            out = dot(hidden, ed[:, lanes(i)])
            yb[k, i] = out.reshape(per_chunk, PAD, quarter).astype(BF16)
            if i:
                remote(
                    yb.at[k, i, :, pl.ds(0, ROWS)],
                    yr.at[k, i, :, pl.ds(0, ROWS)],
                    y_send.at[k],
                    y_recv.at[k],
                    x_peer(i),
                ).start()

    for k in range(EARLY):
        run_expert(k)

    wait_bytes(fac.at[peers_yc], yc_recv.at[2])
    factors = jnp.concatenate(
        [fac[pl.ds(x * per_x + b, 1)][0].T[0:tokens, 0:1] for b in range(per_x)], axis=0
    )
    group_rows = per_x * tokens
    for b in [0] + near_first:
        paired = pr[b, group_of(0)].reshape(group_rows, 2 * units).astype(F32)
        wait_bytes(rs2.at[b, peers_x], r_recv.at[b])
        for i in range(1, n_x):
            paired = paired + rs2[b, i].reshape(group_rows, 2 * units).astype(F32)
        gate, up = paired[:, :units] * factors, paired[:, units:] * factors
        hidden = (silu(gate) * up).astype(BF16)
        hid_all[group_of(0), :, b * units : (b + 1) * units] = hidden.reshape(per_x, tokens, units)
    for i in range(1, n_x):
        remote(
            hid_all.at[group_of(0)],
            hid_all.at[group_of(0)],
            x_send.at[2],
            x_recv.at[2],
            x_peer(i),
        ).start()
    for i in near_first:
        remote(wd.at[0], wd.at[n_z - i], wz_send.at[1], wz_recv.at[0], z_peer(i)).start()

    for k in range(EARLY, CHUNKS):
        run_expert(k)

    def go_home(k):
        out = yb[k, 0].astype(F32)
        wait_bytes(yr.at[k, peers_x, :, pl.ds(0, ROWS)], y_recv.at[k])
        for i in range(1, n_x):
            out = out + yr[k, i].astype(F32)
        rb[chunk(k)] = out.astype(BF16)
        for r in range(k * per_chunk, (k + 1) * per_chunk):
            if r:
                remote(
                    rb.at[r, pl.ds(0, ROWS)],
                    ret.at[r, pl.ds(0, ROWS)],
                    pl_send.at[CHUNKS],
                    pl_recv.at[CHUNKS],
                    ep_at(r, -1),
                ).start()
            else:
                ret[0] = rb[0]

    for k in range(EARLY):
        go_home(k)

    wait_bytes(hid_all.at[pl.ds(0, n_yc - per_x)], x_recv.at[2])

    wait_bytes(wd.at[peers_z], wz_recv.at[0])
    dense_part = dot(
        hid_all[...].reshape(n_yc * tokens, all_units), wd[...].reshape(all_units, quarter)
    )
    db[...] = dense_part.reshape(n_yc, tokens, quarter).astype(BF16)
    for i in range(1, n_yc):
        remote(
            db.at[lax.rem(yc + i, n_yc)], dr.at[i], yc_send.at[1], yc_recv.at[1], yc_peer(i)
        ).start()

    for k in range(EARLY, CHUNKS):
        go_home(k)

    dense = db[pl.ds(yc, 1)][0].astype(F32)
    wait_bytes(dr.at[peers_yc], yc_recv.at[1])
    for i in range(1, n_yc):
        dense = dense + dr[i].astype(F32)

    wait_bytes(ret.at[pl.ds(1, n_ep - 1), pl.ds(0, ROWS)], pl_recv.at[CHUNKS])

    back = ret[...].reshape(n_ep * PAD, quarter)
    routed = turned_dot(comb_hi_ref[...], back) + turned_dot(comb_lo_ref[...], back)
    middle_own = mid[pl.ds(x, 1)][0].astype(F32)
    out_ref[...] = (middle_own + branch * dense + routed).astype(BF16)

    wait_bytes(part.at[peers_x], x_send.at[0])
    wait_bytes(mid.at[peers_x], x_send.at[1])
    wait_bytes(hid_all.at[pl.ds(0, n_yc - per_x)], x_send.at[2])
    for b in range(n_z):
        wait_bytes(rs2.at[b, peers_x], r_send.at[b])
    for k in range(CHUNKS):
        wait_bytes(yb.at[k, peers_x, :, pl.ds(0, ROWS)], y_send.at[k])
    wait_bytes(wgu.at[peers_z], wz_send.at[0])
    wait_bytes(wd.at[peers_z], wz_send.at[1])
    wait_bytes(mid_all.at[peers_yc], yc_send.at[0])
    wait_bytes(db.at[peers_yc], yc_send.at[1])
    wait_bytes(fac.at[peers_yc], yc_send.at[2])
    for k in range(CHUNKS):
        wait_bytes(snd.at[others(k), pl.ds(0, ROWS)], pl_send.at[k])
    wait_bytes(rb.at[pl.ds(1, n_ep - 1), pl.ds(0, ROWS)], pl_send.at[CHUNKS])


def emit_kernel(mixed_ref, state_ref, mixed_hbm, state_hbm, sem):
    step = state_ref.shape[0] // 4
    copies = [pltpu.make_async_copy(mixed_ref, mixed_hbm, sem.at[0])]
    for i in range(4):
        rows = pl.ds(i * step, step)
        copies.append(
            pltpu.make_async_copy(state_ref.at[rows], state_hbm.at[rows], sem.at[1 + i])
        )
    for copy in copies:
        copy.start()
    for copy in copies:
        copy.wait()


def emit(mixed, state):
    vmem = pl.BlockSpec(memory_space=pltpu.VMEM)
    hbm = pl.BlockSpec(memory_space=pltpu.HBM)
    return pl.pallas_call(
        emit_kernel,
        name="emit",
        out_shape=(
            jax.ShapeDtypeStruct(mixed.shape, mixed.dtype),
            jax.ShapeDtypeStruct(state.shape, state.dtype),
        ),
        in_specs=[vmem, vmem],
        out_specs=(hbm, hbm),
        scratch_shapes=[pltpu.SemaphoreType.DMA((5,))],
        compiler_params=pltpu.CompilerParams(vmem_limit_bytes=16 << 20),
    )(mixed, state)


def layer(sizes, small, weights, pw, state, expert, dense):
    n_ep, n_x, n_z = sizes
    n_yc = n_ep // n_z
    tokens, width = small[2].shape
    key_dim, value_dim = state.shape[1:]
    eg, dg = expert[0], dense[0]
    quarter, units = width // n_x, dg.shape[1]
    all_units = n_z * units
    flat = n_ep * PAD
    vmem = pl.BlockSpec(memory_space=pltpu.VMEM)
    hbm = pl.BlockSpec(memory_space=pltpu.HBM)
    dma = pltpu.SemaphoreType.DMA
    operands = (*small, *weights, pw, state, *expert, *dense)
    return pl.pallas_call(
        functools.partial(layer_kernel, sizes),
        name="layer",
        out_shape=(
            jax.ShapeDtypeStruct((tokens, quarter), BF16),
            jax.ShapeDtypeStruct(state.shape, F32),
        ),
        in_specs=[hbm] * len(operands),
        out_specs=(vmem, vmem),
        scratch_shapes=[pltpu.VMEM(a.shape, a.dtype) for a in (*small, *weights, pw)]
        + [
            pltpu.VMEM((tokens, key_dim), F32),
            pltpu.VMEM((tokens, key_dim), F32),
            pltpu.VMEM((tokens, value_dim), F32),
            pltpu.VMEM((tokens, key_dim), F32),
            pltpu.VMEM((tokens, value_dim), F32),
            pltpu.VMEM((n_x, tokens, quarter), BF16),
            pltpu.VMEM((flat, tokens), BF16),
            pltpu.VMEM((flat, tokens), BF16),
            pltpu.VMEM((flat, tokens), BF16),
        ]
        + [pltpu.VMEM(a.shape, a.dtype) for a in expert]
        + [
            pltpu.VMEM((n_z, 2, quarter, units), BF16),
            pltpu.VMEM((n_z, units, quarter), BF16),
            pltpu.VMEM((n_x, tokens, quarter), BF16),
            pltpu.VMEM((n_x, tokens, quarter), BF16),
            pltpu.VMEM((n_ep, PAD, width), BF16),
            pltpu.VMEM((n_ep, PAD, width), BF16),
            pltpu.VMEM((n_yc, tokens, quarter), BF16),
            pltpu.VMEM((tokens, width), BF16),
            pltpu.VMEM((n_yc, 8, 128), F32),
            pltpu.VMEM((n_z, n_yc, tokens, 2 * units), BF16),
            pltpu.VMEM((n_z, n_x, n_yc // n_x, tokens, 2 * units), BF16),
            pltpu.VMEM((n_yc, tokens, all_units), BF16),
            pltpu.VMEM((n_yc, tokens, quarter), BF16),
            pltpu.VMEM((n_yc, tokens, quarter), BF16),
            pltpu.VMEM((CHUNKS, n_x, n_ep // CHUNKS, PAD, quarter), BF16),
            pltpu.VMEM((CHUNKS, n_x, n_ep // CHUNKS, PAD, quarter), BF16),
            pltpu.VMEM((n_ep, PAD, quarter), BF16),
            pltpu.VMEM((n_ep, PAD, quarter), BF16),
            dma((14,)),
            dma((tokens // 8,)),
            dma((6,)),
            dma((2,)),
            dma((n_z,)),
            dma((3,)),
            dma((3,)),
            dma((n_z,)),
            dma((n_z,)),
            dma((CHUNKS,)),
            dma((CHUNKS,)),
            dma((3,)),
            dma((3,)),
            dma((CHUNKS + 1,)),
            dma((CHUNKS + 1,)),
        ],
        compiler_params=pltpu.CompilerParams(
            collective_id=0, has_side_effects=True, vmem_limit_bytes=40 << 20
        ),
    )(*in_hbm(*operands))


def body(
    sizes,
    hidden_in,
    carried_state,
    input_gain,
    query_weight,
    key_weight,
    value_weight,
    outgate_weight,
    decay_weight,
    decay_shift,
    head_gain,
    output_weight,
    channel_gain,
    branch_gate,
    routes,
    route_weights,
    expert_gate,
    expert_up,
    expert_down,
    dense_gate,
    dense_up,
    dense_down,
):
    mixed, new_state = layer(
        sizes,
        (
            routes.T,
            route_weights.T,
            hidden_in,
            input_gain,
            decay_shift,
            head_gain,
            channel_gain,
            branch_gate,
        ),
        (query_weight, key_weight, value_weight, outgate_weight, decay_weight),
        output_weight,
        carried_state[:, 0],
        (expert_gate[0], expert_up[0], expert_down[0]),
        (dense_gate, dense_up, dense_down),
    )
    mixed, new_state = emit(mixed, new_state)
    return (mixed, new_state[:, None])


def solution(mesh):
    in_specs = (
        P("ep", None),
        P("ep", "tp", None, None),
        P(),
        P(None, "tp"),
        P(None, "tp"),
        P(None, "tp"),
        P(None, "tp"),
        P(None, "tp"),
        P("ep", "tp"),
        P("tp", None),
        P("tp", None),
        P(),
        P(),
        P("ep", None),
        P("ep", None),
        P("ep", None, "tp"),
        P("ep", None, "tp"),
        P("ep", "tp", None),
        P("tp", "ep"),
        P("tp", "ep"),
        P("ep", "tp"),
    )
    out_specs = (P("ep", "tp"), P("ep", "tp", None, None))
    n_ep = mesh.shape["ep"]
    sizes = (n_ep, mesh.shape["tp"], min(Z_SIZE, n_ep // 2))
    return jax.shard_map(
        functools.partial(body, sizes),
        mesh=mesh,
        in_specs=in_specs,
        out_specs=out_specs,
        check_vma=False,
    )
```

```python
import functools

import jax
import jax.numpy as jnp
from jax import lax
from jax.experimental import pallas as pl
from jax.experimental.pallas import tpu as pltpu
from jax.sharding import PartitionSpec as P

EPSILON = 1e-06
TAU_DECAY = 16.0
MESH = pl.DeviceIdType.MESH
CAP = 5
ROWS = 6
VMEM_ALL = 67043328
PAD = 8
CHUNKS = 4
EARLY = 2
FLIGHT = 2
GROUP = 16
Z_SIZE = 4
F32 = jnp.float32
BF16 = jnp.bfloat16


def dot(left, right):
    return jnp.dot(left, right, preferred_element_type=F32)


def in_hbm(*arrays):
    return [pltpu.with_memory_space_constraint(a, pltpu.HBM) for a in arrays]


def turned_dot(left, right):
    return lax.dot_general(left, right, (((0,), (0,)), ((), ())), preferred_element_type=F32)


def rms_factor(values):
    return lax.rsqrt(jnp.mean(values * values, axis=-1, keepdims=True) + EPSILON)


def silu(values):
    return values * jax.nn.sigmoid(values)


def layer_kernel(
    sizes,
    routes_hbm,
    rw_hbm,
    hid_hbm,
    gain_hbm,
    shift_hbm,
    hgain_hbm,
    cgain_hbm,
    bgate_hbm,
    qw_hbm,
    kw_hbm,
    vw_hbm,
    ow_hbm,
    dw_hbm,
    pw_hbm,
    state_hbm,
    eg_hbm,
    eu_hbm,
    ed_hbm,
    dg_hbm,
    du_hbm,
    dd_hbm,
    out_ref,
    state_out,
    routes_s,
    rw_s,
    hid_s,
    gain_s,
    shift_s,
    hgain_s,
    cgain_s,
    bgate_s,
    qw,
    kw,
    vw,
    ow,
    dw,
    pw,
    q_s,
    k_s,
    v_s,
    d_s,
    ro_s,
    og_s,
    part,
    sel_ref,
    comb_hi_ref,
    comb_lo_ref,
    eg,
    eu,
    ed,
    wgu,
    wd,
    rs1,
    mid,
    snd,
    rcv,
    mid_all,
    ffn,
    fac,
    pr,
    rs2,
    hid_all,
    db,
    dr,
    yb,
    yr,
    rb,
    ret,
    w_sem,
    in_sem,
    local_sem,
    wz_send,
    wz_recv,
    x_send,
    x_recv,
    r_send,
    r_recv,
    y_send,
    y_recv,
    yc_send,
    yc_recv,
    pl_send,
    pl_recv,
):
    n_ep, n_x, n_z = sizes
    n_yc = n_ep // n_z
    n_y = n_yc // 2
    tokens, width = hid_s.shape
    key_dim = q_s.shape[1]
    groups = tokens // 8
    quarter = width // n_x
    units = dg_hbm.shape[1]
    all_units = n_z * units
    per_chunk = n_ep // CHUNKS
    ep, x = lax.axis_index("ep"), lax.axis_index("tp")
    z, yc = ep // n_yc, ep % n_yc
    y, c = yc // 2, yc % 2

    def x_peer(i):
        return (ep, lax.rem(x + i, n_x))

    def z_peer(i):
        return (lax.rem(z + i, n_z) * n_yc + yc, x)

    def yc_peer(i):
        return (z * n_yc + lax.rem(yc + i, n_yc), x)

    def offsets(r):
        k, j = r // per_chunk, r % per_chunk
        return j // 2, (j % 2) * 2 + k % 2, k // 2

    def ep_at(r, sign):
        dz, dy, dc = offsets(r)
        there_z = lax.rem(z + n_z + sign * dz, n_z)
        there_y = lax.rem(y + n_y + sign * dy, n_y)
        return (there_z * n_yc + there_y * 2 + lax.rem(c + dc, 2), x)

    def remote(src, dst, send, recv, device):
        return pltpu.make_async_remote_copy(
            src_ref=src,
            dst_ref=dst,
            send_sem=send,
            recv_sem=recv,
            device_id=device,
            device_id_type=MESH,
        )

    def lanes(i):
        return pl.ds(pl.multiple_of(lax.rem(x + i, n_x) * quarter, quarter), quarter)

    peers_x, peers_z, peers_yc = pl.ds(1, n_x - 1), pl.ds(1, n_z - 1), pl.ds(1, n_yc - 1)

    def wait_bytes(ref, sem):
        pltpu.make_async_copy(ref, ref, sem).wait()

    small = (
        (routes_hbm, routes_s),
        (rw_hbm, rw_s),
        (hid_hbm, hid_s),
        (gain_hbm, gain_s),
        (shift_hbm, shift_s),
        (hgain_hbm, hgain_s),
        (cgain_hbm, cgain_s),
        (bgate_hbm, bgate_s),
    )
    s_copies = [pltpu.make_async_copy(s, d, w_sem.at[6 + i]) for i, (s, d) in enumerate(small)]
    pairs = ((dw_hbm, dw), (qw_hbm, qw), (kw_hbm, kw), (vw_hbm, vw), (ow_hbm, ow), (pw_hbm, pw))
    w_copies = [pltpu.make_async_copy(s, d, w_sem.at[i]) for i, (s, d) in enumerate(pairs)]
    for copy in s_copies + w_copies[:4]:
        copy.start()

    def state_in(g):
        rows = pl.ds(g * 8, 8)
        return pltpu.make_async_copy(state_hbm.at[rows], state_out.at[rows], in_sem.at[g])

    places = ((dg_hbm, wgu.at[0, 0]), (du_hbm, wgu.at[0, 1]), (dd_hbm, wd.at[0]))
    d_copies = [
        pltpu.make_async_copy(s, d, local_sem.at[3 + i]) for i, (s, d) in enumerate(places)
    ]
    e_copies = [
        pltpu.make_async_copy(s, d, local_sem.at[i])
        for i, (s, d) in enumerate(((eg_hbm, eg), (eu_hbm, eu), (ed_hbm, ed)))
    ]

    rcv[...] = jnp.zeros_like(rcv)
    ret[...] = jnp.zeros_like(ret)
    barrier = pltpu.get_barrier_semaphore()
    for i in range(1, n_x):
        pl.semaphore_signal(barrier, inc=1, device_id=x_peer(i), device_id_type=MESH)
    for r in range(1, n_ep):
        pl.semaphore_signal(barrier, inc=1, device_id=ep_at(r, 1), device_id_type=MESH)
    for copy in d_copies:
        copy.start()
    for g in range(groups):
        state_in(g).start()
    for copy in w_copies[4:]:
        copy.start()

    for copy in s_copies[:2]:
        copy.wait()
    slots = n_ep * PAD
    e_at = lax.broadcasted_iota(jnp.int32, (n_ep, tokens), 0)
    r0, r1 = routes_s[0:1, :], routes_s[1:2, :]
    oh0, oh1 = (e_at == r0).astype(F32), (e_at == r1).astype(F32)
    tri = (
        lax.broadcasted_iota(jnp.int32, (tokens, tokens), 0)
        < lax.broadcasted_iota(jnp.int32, (tokens, tokens), 1)
    ).astype(F32)
    before0 = dot(oh0, tri)
    before1 = dot(oh1, tri) + jnp.sum(oh0, axis=1, keepdims=True)
    slot0 = jnp.sum(before0 * oh0, axis=0, keepdims=True)
    slot1 = jnp.sum(before1 * oh1, axis=0, keepdims=True)

    def place_of(route):
        dz = ((route >> 3) - z) & 3
        dy = (((route >> 1) & 3) - y) & 3
        dc = ((route & 1) - c) & 1
        return (dc * 2 + (dy & 1)) * per_chunk + dz * 2 + (dy >> 1)

    pos0 = place_of(r0) * PAD + slot0.astype(jnp.int32)
    pos1 = place_of(r1) * PAD + slot1.astype(jnp.int32)
    at = lax.broadcasted_iota(jnp.int32, (slots, tokens), 0)
    hit0, hit1 = (at == pos0).astype(F32), (at == pos1).astype(F32)
    sel_ref[...] = (hit0 + hit1).astype(BF16)
    comb = hit0 * rw_s[0:1, :] + hit1 * rw_s[1:2, :]
    comb_hi = comb.astype(BF16)
    comb_hi_ref[...] = comb_hi
    comb_lo_ref[...] = (comb - comb_hi.astype(F32)).astype(BF16)

    for copy in s_copies[2:]:
        copy.wait()
    hid = hid_s[...].astype(F32)
    normed = (hid * rms_factor(hid) * gain_s[...][None, :].astype(F32)).astype(BF16)
    w_copies[0].wait()
    pre = dot(normed, dw[...])
    log_sig = jnp.minimum(pre, 0.0) - jnp.log1p(jnp.exp(-jnp.abs(pre)))
    d_s[...] = jnp.exp(log_sig / TAU_DECAY + shift_s[...])
    w_copies[1].wait()
    q_s[...] = dot(normed, qw[...]).astype(BF16).astype(F32)
    w_copies[2].wait()
    k_s[...] = dot(normed, kw[...]).astype(BF16).astype(F32)
    w_copies[3].wait()
    v_s[...] = dot(normed, vw[...]).astype(BF16).astype(F32)

    for copy in d_copies:
        copy.wait()
    pl.semaphore_wait(barrier, n_x - 1 + n_ep - 1)
    near_first = [1, n_z - 1] + list(range(2, n_z - 1))
    for i in near_first:
        b = n_z - i
        remote(wgu.at[0], wgu.at[b], wz_send.at[0], wz_recv.at[b], z_peer(i)).start()

    span = GROUP * key_dim
    at_block = lax.broadcasted_iota(jnp.int32, (GROUP, span), 1) // key_dim
    on_block = at_block == lax.broadcasted_iota(jnp.int32, (GROUP, span), 0)

    def spread(rows):
        return jnp.where(on_block, jnp.concatenate([rows] * GROUP, axis=1), 0.0).astype(BF16)

    def group(g, carry):
        for part_of in range(GROUP // 8):
            state_in(g * (GROUP // 8) + part_of).wait()
        rows = pl.ds(pl.multiple_of(g * GROUP, GROUP), GROUP)
        d_t = d_s[rows, :].T
        outer = turned_dot(spread(k_s[rows, :]), v_s[rows, :].astype(BF16))
        news = []
        for j in range(GROUP):
            b = g * GROUP + j
            added = outer[j * key_dim : (j + 1) * key_dim, :]
            new = d_t[:, j : j + 1] * state_out[b] + added
            state_out[b] = new
            news.append(new.astype(BF16))
        ro_s[rows, :] = dot(spread(q_s[rows, :]), jnp.concatenate(news, axis=0))
        return carry

    cut = tokens - GROUP
    parts = (slice(0, cut), slice(cut, tokens))

    def rows_of(p):
        return pl.ds(parts[p].start, parts[p].stop - parts[p].start)

    def send_heads(p):
        readout = ro_s[parts[p], :] * key_dim ** (-0.5)
        gated = readout * rms_factor(readout) * hgain_s[...].astype(F32) * og_s[parts[p], :]
        gated = gated.astype(BF16)
        for i in range(1, n_x):
            part[i, parts[p]] = dot(gated, pw[:, lanes(i)]).astype(BF16)
            remote(
                part.at[i, rows_of(p)],
                rs1.at[i, rows_of(p)],
                x_send.at[p],
                x_recv.at[p],
                x_peer(i),
            ).start()
        return dot(gated, pw[:, lanes(0)]).astype(BF16).astype(F32)

    def send_middle(p, total):
        wait_bytes(rs1.at[peers_x, rows_of(p)], x_recv.at[p])
        for i in range(1, n_x):
            total = total + rs1[i, parts[p]].astype(F32)
        middle_q = (hid_s[parts[p], lanes(0)].astype(F32) + total).astype(BF16)
        mid[pl.ds(x, 1), parts[p]] = middle_q[None]
        mid_all[pl.ds(yc, 1), parts[p]] = middle_q[None]
        for i in range(1, n_x):
            mine = mid.at[x, rows_of(p)]
            remote(mine, mine, x_send.at[2 + p], x_recv.at[2 + p], x_peer(i)).start()
        for i in range(1, n_yc):
            mine = mid_all.at[yc, rows_of(p)]
            remote(mine, mine, yc_send.at[p], yc_recv.at[p], yc_peer(i)).start()

    lax.fori_loop(0, cut // GROUP, group, 0)

    w_copies[4].wait()
    og_s[...] = silu(dot(normed, ow[...]).astype(BF16).astype(F32))
    w_copies[5].wait()
    total_1 = send_heads(0)

    lax.fori_loop(cut // GROUP, tokens // GROUP, group, 0)

    total_2 = send_heads(1)
    for copy in e_copies:
        copy.start()

    send_middle(0, total_1)

    send_middle(1, total_2)

    for p in range(2):
        wait_bytes(mid.at[peers_x, rows_of(p)], x_recv.at[2 + p])

    squares = sum(
        jnp.sum(mid[i].astype(F32) * mid[i].astype(F32), axis=-1, keepdims=True) for i in range(n_x)
    )
    factor = lax.rsqrt(squares / width + EPSILON)
    logit = jnp.zeros((tokens, 1), F32)
    for i in range(n_x):
        cols = slice(i * quarter, (i + 1) * quarter)
        scaled = mid[i].astype(F32) * factor * cgain_s[cols][None, :].astype(F32)
        logit = logit + jnp.sum(scaled * bgate_s[cols][None, :].astype(F32), axis=-1, keepdims=True)
        ffn[:, cols] = scaled.astype(BF16)
    branch = jax.nn.sigmoid(logit)

    def chunk(k):
        return pl.ds(k * per_chunk, per_chunk)

    def others(k):
        first = 1 if k == 0 else 0
        return pl.ds(k * per_chunk + first, per_chunk - first)

    def dispatch(k):
        for r in range(k * per_chunk, (k + 1) * per_chunk):
            if r:
                remote(
                    snd.at[r, pl.ds(0, ROWS)],
                    rcv.at[r, pl.ds(0, ROWS)],
                    pl_send.at[k],
                    pl_recv.at[k],
                    ep_at(r, 1),
                ).start()

    for k in range(CHUNKS):
        rows = dot(sel_ref[k * per_chunk * PAD : (k + 1) * per_chunk * PAD, :], ffn[...])
        snd[chunk(k)] = rows.reshape(per_chunk, PAD, width).astype(BF16)
        if k < FLIGHT:
            dispatch(k)
    rcv[0] = snd[0]
    factor_rows = jnp.broadcast_to(factor, (tokens, 128)).T[0:8, :]
    fac[pl.ds(yc, 1), :, 0:tokens] = factor_rows[None]
    for i in range(1, n_yc):
        remote(fac.at[yc], fac.at[yc], yc_send.at[3], yc_recv.at[3], yc_peer(i)).start()

    for p in range(2):
        wait_bytes(mid_all.at[peers_yc, rows_of(p)], yc_recv.at[p])

    per_x = n_yc // n_x
    gain_q = cgain_s[lanes(0)][None, :].astype(F32)
    rows_in = mid_all[...].reshape(n_yc * tokens, quarter).astype(F32) * gain_q
    rows_in = rows_in.astype(BF16)

    def group_of(i):
        return pl.ds(lax.rem(x + i, n_x) * per_x, per_x)

    def gate_up(b):
        paired = dot(rows_in, jnp.concatenate([wgu[b, 0], wgu[b, 1]], axis=1))
        pr[b] = paired.astype(BF16).reshape(n_yc, tokens, 2 * units)
        for i in range(1, n_x):
            remote(
                pr.at[b, group_of(i)], rs2.at[b, i], r_send.at[b], r_recv.at[b], x_peer(i)
            ).start()

    gate_up(0)

    for b in near_first:
        wait_bytes(wgu.at[b], wz_recv.at[b])
        gate_up(b)

    for copy in e_copies:
        copy.wait()
    flat = per_chunk * PAD

    def run_expert(k):
        wait_bytes(rcv.at[others(k), pl.ds(0, ROWS)], pl_recv.at[k])
        if k + FLIGHT < CHUNKS:
            dispatch(k + FLIGHT)
            if k + FLIGHT == CHUNKS - 1:
                for i in near_first:
                    b = n_z - i
                    remote(wd.at[0], wd.at[b], wz_send.at[1], wz_recv.at[0], z_peer(i)).start()
        rows = rcv[chunk(k)].reshape(flat, width)
        hidden = (silu(dot(rows, eg[...])) * dot(rows, eu[...])).astype(BF16)
        for i in list(range(1, n_x)) + [0]:
            out = dot(hidden, ed[:, lanes(i)])
            yb[k, i] = out.reshape(per_chunk, PAD, quarter).astype(BF16)
            if i:
                remote(
                    yb.at[k, i, :, pl.ds(0, ROWS)],
                    yr.at[k, i, :, pl.ds(0, ROWS)],
                    y_send.at[k],
                    y_recv.at[k],
                    x_peer(i),
                ).start()

    for k in range(EARLY):
        run_expert(k)

    wait_bytes(fac.at[peers_yc], yc_recv.at[3])
    factors = jnp.concatenate(
        [fac[pl.ds(x * per_x + b, 1)][0].T[0:tokens, 0:1] for b in range(per_x)], axis=0
    )
    group_rows = per_x * tokens
    for b in [0] + near_first:
        paired = pr[b, group_of(0)].reshape(group_rows, 2 * units).astype(F32)
        wait_bytes(rs2.at[b, peers_x], r_recv.at[b])
        for i in range(1, n_x):
            paired = paired + rs2[b, i].reshape(group_rows, 2 * units).astype(F32)
        gate, up = paired[:, :units] * factors, paired[:, units:] * factors
        hidden = (silu(gate) * up).astype(BF16)
        hid_all[group_of(0), :, b * units : (b + 1) * units] = hidden.reshape(per_x, tokens, units)
    for i in range(1, n_x):
        remote(
            hid_all.at[group_of(0)],
            hid_all.at[group_of(0)],
            x_send.at[4],
            x_recv.at[4],
            x_peer(i),
        ).start()

    for k in range(EARLY, CHUNKS):
        run_expert(k)

    def go_home(k):
        out = yb[k, 0].astype(F32)
        wait_bytes(yr.at[k, peers_x, :, pl.ds(0, ROWS)], y_recv.at[k])
        for i in range(1, n_x):
            out = out + yr[k, i].astype(F32)
        rb[chunk(k)] = out.astype(BF16)
        for r in range(k * per_chunk, (k + 1) * per_chunk):
            if r:
                remote(
                    rb.at[r, pl.ds(0, ROWS)],
                    ret.at[r, pl.ds(0, ROWS)],
                    pl_send.at[CHUNKS],
                    pl_recv.at[CHUNKS],
                    ep_at(r, -1),
                ).start()
            else:
                ret[0] = rb[0]

    for k in range(EARLY):
        go_home(k)

    wait_bytes(hid_all.at[pl.ds(0, n_yc - per_x)], x_recv.at[4])

    wait_bytes(wd.at[peers_z], wz_recv.at[0])
    dense_part = dot(
        hid_all[...].reshape(n_yc * tokens, all_units), wd[...].reshape(all_units, quarter)
    )
    db[...] = dense_part.reshape(n_yc, tokens, quarter).astype(BF16)
    for i in range(1, n_yc):
        remote(
            db.at[lax.rem(yc + i, n_yc)], dr.at[i], yc_send.at[2], yc_recv.at[2], yc_peer(i)
        ).start()

    for k in range(EARLY, CHUNKS):
        go_home(k)

    dense = db[pl.ds(yc, 1)][0].astype(F32)
    wait_bytes(dr.at[peers_yc], yc_recv.at[2])
    for i in range(1, n_yc):
        dense = dense + dr[i].astype(F32)

    wait_bytes(ret.at[pl.ds(1, n_ep - 1), pl.ds(0, ROWS)], pl_recv.at[CHUNKS])

    back = ret[...].reshape(n_ep * PAD, quarter)
    routed = turned_dot(comb_hi_ref[...], back) + turned_dot(comb_lo_ref[...], back)
    middle_own = mid[pl.ds(x, 1)][0].astype(F32)
    out_ref[...] = (middle_own + branch * dense + routed).astype(BF16)

    for p in range(2):
        wait_bytes(part.at[peers_x, rows_of(p)], x_send.at[p])
        wait_bytes(mid.at[peers_x, rows_of(p)], x_send.at[2 + p])
        wait_bytes(mid_all.at[peers_yc, rows_of(p)], yc_send.at[p])
    wait_bytes(hid_all.at[pl.ds(0, n_yc - per_x)], x_send.at[4])
    for b in range(n_z):
        wait_bytes(rs2.at[b, peers_x], r_send.at[b])
    for k in range(CHUNKS):
        wait_bytes(yb.at[k, peers_x, :, pl.ds(0, ROWS)], y_send.at[k])
    wait_bytes(wgu.at[peers_z], wz_send.at[0])
    wait_bytes(wd.at[peers_z], wz_send.at[1])
    wait_bytes(db.at[peers_yc], yc_send.at[2])
    wait_bytes(fac.at[peers_yc], yc_send.at[3])
    for k in range(CHUNKS):
        wait_bytes(snd.at[others(k), pl.ds(0, ROWS)], pl_send.at[k])
    wait_bytes(rb.at[pl.ds(1, n_ep - 1), pl.ds(0, ROWS)], pl_send.at[CHUNKS])


def emit_kernel(mixed_ref, state_ref, mixed_hbm, state_hbm, sem):
    step = state_ref.shape[0] // 4
    copies = [pltpu.make_async_copy(mixed_ref, mixed_hbm, sem.at[0])]
    for i in range(4):
        rows = pl.ds(i * step, step)
        copies.append(
            pltpu.make_async_copy(state_ref.at[rows], state_hbm.at[rows], sem.at[1 + i])
        )
    for copy in copies:
        copy.start()
    for copy in copies:
        copy.wait()


def emit(mixed, state):
    vmem = pl.BlockSpec(memory_space=pltpu.VMEM)
    hbm = pl.BlockSpec(memory_space=pltpu.HBM)
    return pl.pallas_call(
        emit_kernel,
        name="emit",
        out_shape=(
            jax.ShapeDtypeStruct(mixed.shape, mixed.dtype),
            jax.ShapeDtypeStruct(state.shape, state.dtype),
        ),
        in_specs=[vmem, vmem],
        out_specs=(hbm, hbm),
        scratch_shapes=[pltpu.SemaphoreType.DMA((5,))],
        compiler_params=pltpu.CompilerParams(vmem_limit_bytes=16 << 20),
    )(mixed, state)


def layer(sizes, small, weights, pw, state, expert, dense):
    n_ep, n_x, n_z = sizes
    n_yc = n_ep // n_z
    tokens, width = small[2].shape
    key_dim, value_dim = state.shape[1:]
    eg, dg = expert[0], dense[0]
    quarter, units = width // n_x, dg.shape[1]
    all_units = n_z * units
    flat = n_ep * PAD
    vmem = pl.BlockSpec(memory_space=pltpu.VMEM)
    hbm = pl.BlockSpec(memory_space=pltpu.HBM)
    dma = pltpu.SemaphoreType.DMA
    operands = (*small, *weights, pw, state, *expert, *dense)
    return pl.pallas_call(
        functools.partial(layer_kernel, sizes),
        name="layer",
        out_shape=(
            jax.ShapeDtypeStruct((tokens, quarter), BF16),
            jax.ShapeDtypeStruct(state.shape, F32),
        ),
        in_specs=[hbm] * len(operands),
        out_specs=(vmem, vmem),
        scratch_shapes=[pltpu.VMEM(a.shape, a.dtype) for a in (*small, *weights, pw)]
        + [
            pltpu.VMEM((tokens, key_dim), F32),
            pltpu.VMEM((tokens, key_dim), F32),
            pltpu.VMEM((tokens, value_dim), F32),
            pltpu.VMEM((tokens, key_dim), F32),
            pltpu.VMEM((tokens, value_dim), F32),
            pltpu.VMEM((tokens, value_dim), F32),
            pltpu.VMEM((n_x, tokens, quarter), BF16),
            pltpu.VMEM((flat, tokens), BF16),
            pltpu.VMEM((flat, tokens), BF16),
            pltpu.VMEM((flat, tokens), BF16),
        ]
        + [pltpu.VMEM(a.shape, a.dtype) for a in expert]
        + [
            pltpu.VMEM((n_z, 2, quarter, units), BF16),
            pltpu.VMEM((n_z, units, quarter), BF16),
            pltpu.VMEM((n_x, tokens, quarter), BF16),
            pltpu.VMEM((n_x, tokens, quarter), BF16),
            pltpu.VMEM((n_ep, PAD, width), BF16),
            pltpu.VMEM((n_ep, PAD, width), BF16),
            pltpu.VMEM((n_yc, tokens, quarter), BF16),
            pltpu.VMEM((tokens, width), BF16),
            pltpu.VMEM((n_yc, 8, 128), F32),
            pltpu.VMEM((n_z, n_yc, tokens, 2 * units), BF16),
            pltpu.VMEM((n_z, n_x, n_yc // n_x, tokens, 2 * units), BF16),
            pltpu.VMEM((n_yc, tokens, all_units), BF16),
            pltpu.VMEM((n_yc, tokens, quarter), BF16),
            pltpu.VMEM((n_yc, tokens, quarter), BF16),
            pltpu.VMEM((CHUNKS, n_x, n_ep // CHUNKS, PAD, quarter), BF16),
            pltpu.VMEM((CHUNKS, n_x, n_ep // CHUNKS, PAD, quarter), BF16),
            pltpu.VMEM((n_ep, PAD, quarter), BF16),
            pltpu.VMEM((n_ep, PAD, quarter), BF16),
            dma((14,)),
            dma((tokens // 8,)),
            dma((6,)),
            dma((2,)),
            dma((n_z,)),
            dma((5,)),
            dma((5,)),
            dma((n_z,)),
            dma((n_z,)),
            dma((CHUNKS,)),
            dma((CHUNKS,)),
            dma((4,)),
            dma((4,)),
            dma((CHUNKS + 1,)),
            dma((CHUNKS + 1,)),
        ],
        compiler_params=pltpu.CompilerParams(
            collective_id=0, has_side_effects=True, vmem_limit_bytes=40 << 20
        ),
    )(*in_hbm(*operands))


def body(
    sizes,
    hidden_in,
    carried_state,
    input_gain,
    query_weight,
    key_weight,
    value_weight,
    outgate_weight,
    decay_weight,
    decay_shift,
    head_gain,
    output_weight,
    channel_gain,
    branch_gate,
    routes,
    route_weights,
    expert_gate,
    expert_up,
    expert_down,
    dense_gate,
    dense_up,
    dense_down,
):
    mixed, new_state = layer(
        sizes,
        (
            routes.T,
            route_weights.T,
            hidden_in,
            input_gain,
            decay_shift,
            head_gain,
            channel_gain,
            branch_gate,
        ),
        (query_weight, key_weight, value_weight, outgate_weight, decay_weight),
        output_weight,
        carried_state[:, 0],
        (expert_gate[0], expert_up[0], expert_down[0]),
        (dense_gate, dense_up, dense_down),
    )
    mixed, new_state = emit(mixed, new_state)
    return (mixed, new_state[:, None])


def solution(mesh):
    in_specs = (
        P("ep", None),
        P("ep", "tp", None, None),
        P(),
        P(None, "tp"),
        P(None, "tp"),
        P(None, "tp"),
        P(None, "tp"),
        P(None, "tp"),
        P("ep", "tp"),
        P("tp", None),
        P("tp", None),
        P(),
        P(),
        P("ep", None),
        P("ep", None),
        P("ep", None, "tp"),
        P("ep", None, "tp"),
        P("ep", "tp", None),
        P("tp", "ep"),
        P("tp", "ep"),
        P("ep", "tp"),
    )
    out_specs = (P("ep", "tp"), P("ep", "tp", None, None))
    n_ep = mesh.shape["ep"]
    sizes = (n_ep, mesh.shape["tp"], min(Z_SIZE, n_ep // 2))
    return jax.shard_map(
        functools.partial(body, sizes),
        mesh=mesh,
        in_specs=in_specs,
        out_specs=out_specs,
        check_vma=False,
    )
```

```python
import functools

import jax
import jax.numpy as jnp
from jax import lax
from jax.experimental import pallas as pl
from jax.experimental.pallas import tpu as pltpu
from jax.sharding import PartitionSpec as P

EPSILON = 1e-06
TAU_DECAY = 16.0
MESH = pl.DeviceIdType.MESH
CAP = 5
ROWS = 6
VMEM_ALL = 67043328
PAD = 8
CHUNKS = 4
EARLY = 2
FLIGHT = 2
GROUP = 16
Z_SIZE = 4
F32 = jnp.float32
BF16 = jnp.bfloat16


def dot(left, right):
    return jnp.dot(left, right, preferred_element_type=F32)


def in_hbm(*arrays):
    return [pltpu.with_memory_space_constraint(a, pltpu.HBM) for a in arrays]


def turned_dot(left, right):
    return lax.dot_general(left, right, (((0,), (0,)), ((), ())), preferred_element_type=F32)


def rms_factor(values):
    return lax.rsqrt(jnp.mean(values * values, axis=-1, keepdims=True) + EPSILON)


def silu(values):
    return values * jax.nn.sigmoid(values)


def layer_kernel(
    sizes,
    routes_hbm,
    rw_hbm,
    hid_hbm,
    gain_hbm,
    shift_hbm,
    hgain_hbm,
    cgain_hbm,
    bgate_hbm,
    qw_hbm,
    kw_hbm,
    vw_hbm,
    ow_hbm,
    dw_hbm,
    pw_hbm,
    state_hbm,
    eg_hbm,
    eu_hbm,
    ed_hbm,
    dg_hbm,
    du_hbm,
    dd_hbm,
    out_ref,
    state_out,
    routes_s,
    rw_s,
    hid_s,
    gain_s,
    shift_s,
    hgain_s,
    cgain_s,
    bgate_s,
    qw,
    kw,
    vw,
    ow,
    dw,
    pw,
    q_s,
    k_s,
    v_s,
    d_s,
    ro_s,
    og_s,
    part,
    sel_ref,
    comb_hi_ref,
    comb_lo_ref,
    eg,
    eu,
    ed,
    wgu,
    wd,
    rs1,
    mid,
    snd,
    rcv,
    mid_all,
    ffn,
    fac,
    pr,
    rs2,
    hid_all,
    db,
    dr,
    yb,
    yr,
    rb,
    ret,
    w_sem,
    in_sem,
    local_sem,
    wz_send,
    wz_recv,
    x_send,
    x_recv,
    r_send,
    r_recv,
    y_send,
    y_recv,
    yc_send,
    yc_recv,
    pl_send,
    pl_recv,
):
    n_ep, n_x, n_z = sizes
    n_yc = n_ep // n_z
    n_y = n_yc // 2
    tokens, width = hid_s.shape
    key_dim = q_s.shape[1]
    groups = tokens // 8
    quarter = width // n_x
    units = dg_hbm.shape[1]
    all_units = n_z * units
    per_chunk = n_ep // CHUNKS
    ep, x = lax.axis_index("ep"), lax.axis_index("tp")
    z, yc = ep // n_yc, ep % n_yc
    y, c = yc // 2, yc % 2

    def x_peer(i):
        return (ep, lax.rem(x + i, n_x))

    def z_peer(i):
        return (lax.rem(z + i, n_z) * n_yc + yc, x)

    def yc_peer(i):
        return (z * n_yc + lax.rem(yc + i, n_yc), x)

    def offsets(r):
        k, j = r // per_chunk, r % per_chunk
        return j // 2, (j % 2) * 2 + k % 2, k // 2

    def ep_at(r, sign):
        dz, dy, dc = offsets(r)
        there_z = lax.rem(z + n_z + sign * dz, n_z)
        there_y = lax.rem(y + n_y + sign * dy, n_y)
        return (there_z * n_yc + there_y * 2 + lax.rem(c + dc, 2), x)

    def remote(src, dst, send, recv, device):
        return pltpu.make_async_remote_copy(
            src_ref=src,
            dst_ref=dst,
            send_sem=send,
            recv_sem=recv,
            device_id=device,
            device_id_type=MESH,
        )

    def lanes(i):
        return pl.ds(pl.multiple_of(lax.rem(x + i, n_x) * quarter, quarter), quarter)

    peers_x, peers_z, peers_yc = pl.ds(1, n_x - 1), pl.ds(1, n_z - 1), pl.ds(1, n_yc - 1)

    def wait_bytes(ref, sem):
        pltpu.make_async_copy(ref, ref, sem).wait()

    small = (
        (routes_hbm, routes_s),
        (rw_hbm, rw_s),
        (hid_hbm, hid_s),
        (gain_hbm, gain_s),
        (shift_hbm, shift_s),
        (hgain_hbm, hgain_s),
        (cgain_hbm, cgain_s),
        (bgate_hbm, bgate_s),
    )
    s_copies = [pltpu.make_async_copy(s, d, w_sem.at[6 + i]) for i, (s, d) in enumerate(small)]
    pairs = ((dw_hbm, dw), (qw_hbm, qw), (kw_hbm, kw), (vw_hbm, vw), (ow_hbm, ow), (pw_hbm, pw))
    w_copies = [pltpu.make_async_copy(s, d, w_sem.at[i]) for i, (s, d) in enumerate(pairs)]
    for copy in s_copies + w_copies[:4]:
        copy.start()

    def state_in(g):
        rows = pl.ds(g * 8, 8)
        return pltpu.make_async_copy(state_hbm.at[rows], state_out.at[rows], in_sem.at[g])

    places = ((dg_hbm, wgu.at[0, 0]), (du_hbm, wgu.at[0, 1]), (dd_hbm, wd.at[0]))
    d_copies = [
        pltpu.make_async_copy(s, d, local_sem.at[3 + i]) for i, (s, d) in enumerate(places)
    ]
    e_copies = [
        pltpu.make_async_copy(s, d, local_sem.at[i])
        for i, (s, d) in enumerate(((eg_hbm, eg), (eu_hbm, eu), (ed_hbm, ed)))
    ]

    rcv[...] = jnp.zeros_like(rcv)
    ret[...] = jnp.zeros_like(ret)
    barrier = pltpu.get_barrier_semaphore()
    for i in range(1, n_x):
        pl.semaphore_signal(barrier, inc=1, device_id=x_peer(i), device_id_type=MESH)
    for r in range(1, n_ep):
        pl.semaphore_signal(barrier, inc=1, device_id=ep_at(r, 1), device_id_type=MESH)
    for copy in d_copies:
        copy.start()
    for g in range(groups):
        state_in(g).start()
    for copy in w_copies[4:]:
        copy.start()

    for copy in s_copies[:2]:
        copy.wait()
    slots = n_ep * PAD
    e_at = lax.broadcasted_iota(jnp.int32, (n_ep, tokens), 0)
    r0, r1 = routes_s[0:1, :], routes_s[1:2, :]
    oh0, oh1 = (e_at == r0).astype(F32), (e_at == r1).astype(F32)
    tri = (
        lax.broadcasted_iota(jnp.int32, (tokens, tokens), 0)
        < lax.broadcasted_iota(jnp.int32, (tokens, tokens), 1)
    ).astype(F32)
    before0 = dot(oh0, tri)
    before1 = dot(oh1, tri) + jnp.sum(oh0, axis=1, keepdims=True)
    slot0 = jnp.sum(before0 * oh0, axis=0, keepdims=True)
    slot1 = jnp.sum(before1 * oh1, axis=0, keepdims=True)

    def place_of(route):
        dz = ((route >> 3) - z) & 3
        dy = (((route >> 1) & 3) - y) & 3
        dc = ((route & 1) - c) & 1
        return (dc * 2 + (dy & 1)) * per_chunk + dz * 2 + (dy >> 1)

    pos0 = place_of(r0) * PAD + slot0.astype(jnp.int32)
    pos1 = place_of(r1) * PAD + slot1.astype(jnp.int32)
    at = lax.broadcasted_iota(jnp.int32, (slots, tokens), 0)
    hit0, hit1 = (at == pos0).astype(F32), (at == pos1).astype(F32)
    sel_ref[...] = (hit0 + hit1).astype(BF16)
    comb = hit0 * rw_s[0:1, :] + hit1 * rw_s[1:2, :]
    comb_hi = comb.astype(BF16)
    comb_hi_ref[...] = comb_hi
    comb_lo_ref[...] = (comb - comb_hi.astype(F32)).astype(BF16)

    for copy in s_copies[2:]:
        copy.wait()
    hid = hid_s[...].astype(F32)
    normed = (hid * rms_factor(hid) * gain_s[...][None, :].astype(F32)).astype(BF16)
    w_copies[0].wait()
    pre = dot(normed, dw[...])
    log_sig = jnp.minimum(pre, 0.0) - jnp.log1p(jnp.exp(-jnp.abs(pre)))
    d_s[...] = jnp.exp(log_sig / TAU_DECAY + shift_s[...])
    w_copies[1].wait()
    q_s[...] = dot(normed, qw[...]).astype(BF16).astype(F32)
    w_copies[2].wait()
    k_s[...] = dot(normed, kw[...]).astype(BF16).astype(F32)
    w_copies[3].wait()
    v_s[...] = dot(normed, vw[...]).astype(BF16).astype(F32)

    span = GROUP * key_dim
    at_block = lax.broadcasted_iota(jnp.int32, (GROUP, span), 1) // key_dim
    on_block = at_block == lax.broadcasted_iota(jnp.int32, (GROUP, span), 0)

    def spread(rows):
        return jnp.where(on_block, jnp.concatenate([rows] * GROUP, axis=1), 0.0).astype(BF16)

    def group(g, carry):
        for part_of in range(GROUP // 8):
            state_in(g * (GROUP // 8) + part_of).wait()
        rows = pl.ds(pl.multiple_of(g * GROUP, GROUP), GROUP)
        d_t = d_s[rows, :].T
        outer = turned_dot(spread(k_s[rows, :]), v_s[rows, :].astype(BF16))
        news = []
        for j in range(GROUP):
            b = g * GROUP + j
            added = outer[j * key_dim : (j + 1) * key_dim, :]
            new = d_t[:, j : j + 1] * state_out[b] + added
            state_out[b] = new
            news.append(new.astype(BF16))
        ro_s[rows, :] = dot(spread(q_s[rows, :]), jnp.concatenate(news, axis=0))
        return carry

    cut = tokens - GROUP
    parts = (slice(0, cut), slice(cut, tokens))

    def rows_of(p):
        return pl.ds(parts[p].start, parts[p].stop - parts[p].start)

    def send_heads(p):
        readout = ro_s[parts[p], :] * key_dim ** (-0.5)
        gated = readout * rms_factor(readout) * hgain_s[...].astype(F32) * og_s[parts[p], :]
        gated = gated.astype(BF16)
        for i in range(1, n_x):
            part[i, parts[p]] = dot(gated, pw[:, lanes(i)]).astype(BF16)
            remote(
                part.at[i, rows_of(p)],
                rs1.at[i, rows_of(p)],
                x_send.at[p],
                x_recv.at[p],
                x_peer(i),
            ).start()
        return dot(gated, pw[:, lanes(0)]).astype(BF16).astype(F32)

    def send_middle(p, total):
        wait_bytes(rs1.at[peers_x, rows_of(p)], x_recv.at[p])
        for i in range(1, n_x):
            total = total + rs1[i, parts[p]].astype(F32)
        middle_q = (hid_s[parts[p], lanes(0)].astype(F32) + total).astype(BF16)
        mid[pl.ds(x, 1), parts[p]] = middle_q[None]
        mid_all[pl.ds(yc, 1), parts[p]] = middle_q[None]
        for i in range(1, n_x):
            mine = mid.at[x, rows_of(p)]
            remote(mine, mine, x_send.at[2 + p], x_recv.at[2 + p], x_peer(i)).start()
        for i in range(1, n_yc):
            mine = mid_all.at[yc, rows_of(p)]
            remote(mine, mine, yc_send.at[p], yc_recv.at[p], yc_peer(i)).start()

    lax.fori_loop(0, cut // GROUP, group, 0)

    for copy in d_copies:
        copy.wait()
    pl.semaphore_wait(barrier, n_x - 1 + n_ep - 1)
    near_first = [1, n_z - 1] + list(range(2, n_z - 1))
    for i in near_first:
        b = n_z - i
        remote(wgu.at[0], wgu.at[b], wz_send.at[0], wz_recv.at[b], z_peer(i)).start()

    w_copies[4].wait()
    og_s[...] = silu(dot(normed, ow[...]).astype(BF16).astype(F32))
    w_copies[5].wait()
    total_1 = send_heads(0)

    lax.fori_loop(cut // GROUP, tokens // GROUP, group, 0)

    total_2 = send_heads(1)
    for copy in e_copies:
        copy.start()

    send_middle(0, total_1)

    send_middle(1, total_2)

    for p in range(2):
        wait_bytes(mid.at[peers_x, rows_of(p)], x_recv.at[2 + p])

    squares = sum(
        jnp.sum(mid[i].astype(F32) * mid[i].astype(F32), axis=-1, keepdims=True) for i in range(n_x)
    )
    factor = lax.rsqrt(squares / width + EPSILON)
    logit = jnp.zeros((tokens, 1), F32)
    for i in range(n_x):
        cols = slice(i * quarter, (i + 1) * quarter)
        scaled = mid[i].astype(F32) * factor * cgain_s[cols][None, :].astype(F32)
        logit = logit + jnp.sum(scaled * bgate_s[cols][None, :].astype(F32), axis=-1, keepdims=True)
        ffn[:, cols] = scaled.astype(BF16)
    branch = jax.nn.sigmoid(logit)

    def chunk(k):
        return pl.ds(k * per_chunk, per_chunk)

    def others(k):
        first = 1 if k == 0 else 0
        return pl.ds(k * per_chunk + first, per_chunk - first)

    def dispatch(k):
        for r in range(k * per_chunk, (k + 1) * per_chunk):
            if r:
                remote(
                    snd.at[r, pl.ds(0, ROWS)],
                    rcv.at[r, pl.ds(0, ROWS)],
                    pl_send.at[k],
                    pl_recv.at[k],
                    ep_at(r, 1),
                ).start()

    for k in range(CHUNKS):
        rows = dot(sel_ref[k * per_chunk * PAD : (k + 1) * per_chunk * PAD, :], ffn[...])
        snd[chunk(k)] = rows.reshape(per_chunk, PAD, width).astype(BF16)
        if k < FLIGHT:
            dispatch(k)
    rcv[0] = snd[0]
    factor_rows = jnp.broadcast_to(factor, (tokens, 128)).T[0:8, :]
    fac[pl.ds(yc, 1), :, 0:tokens] = factor_rows[None]
    for i in range(1, n_yc):
        remote(fac.at[yc], fac.at[yc], yc_send.at[3], yc_recv.at[3], yc_peer(i)).start()

    for p in range(2):
        wait_bytes(mid_all.at[peers_yc, rows_of(p)], yc_recv.at[p])

    per_x = n_yc // n_x
    gain_q = cgain_s[lanes(0)][None, :].astype(F32)
    rows_in = mid_all[...].reshape(n_yc * tokens, quarter).astype(F32) * gain_q
    rows_in = rows_in.astype(BF16)

    def group_of(i):
        return pl.ds(lax.rem(x + i, n_x) * per_x, per_x)

    def gate_up(b):
        paired = dot(rows_in, jnp.concatenate([wgu[b, 0], wgu[b, 1]], axis=1))
        pr[b] = paired.astype(BF16).reshape(n_yc, tokens, 2 * units)
        for i in range(1, n_x):
            remote(
                pr.at[b, group_of(i)], rs2.at[b, i], r_send.at[b], r_recv.at[b], x_peer(i)
            ).start()

    gate_up(0)

    for b in near_first:
        wait_bytes(wgu.at[b], wz_recv.at[b])
        gate_up(b)

    for copy in e_copies:
        copy.wait()
    flat = per_chunk * PAD

    def run_expert(k):
        wait_bytes(rcv.at[others(k), pl.ds(0, ROWS)], pl_recv.at[k])
        if k + FLIGHT < CHUNKS:
            dispatch(k + FLIGHT)
            if k + FLIGHT == CHUNKS - 1:
                for i in near_first:
                    b = n_z - i
                    remote(wd.at[0], wd.at[b], wz_send.at[1], wz_recv.at[0], z_peer(i)).start()
        rows = rcv[chunk(k)].reshape(flat, width)
        hidden = (silu(dot(rows, eg[...])) * dot(rows, eu[...])).astype(BF16)
        for i in list(range(1, n_x)) + [0]:
            out = dot(hidden, ed[:, lanes(i)])
            yb[k, i] = out.reshape(per_chunk, PAD, quarter).astype(BF16)
            if i:
                remote(
                    yb.at[k, i, :, pl.ds(0, ROWS)],
                    yr.at[k, i, :, pl.ds(0, ROWS)],
                    y_send.at[k],
                    y_recv.at[k],
                    x_peer(i),
                ).start()

    for k in range(EARLY):
        run_expert(k)

    wait_bytes(fac.at[peers_yc], yc_recv.at[3])
    factors = jnp.concatenate(
        [fac[pl.ds(x * per_x + b, 1)][0].T[0:tokens, 0:1] for b in range(per_x)], axis=0
    )
    group_rows = per_x * tokens
    for b in [0] + near_first:
        paired = pr[b, group_of(0)].reshape(group_rows, 2 * units).astype(F32)
        wait_bytes(rs2.at[b, peers_x], r_recv.at[b])
        for i in range(1, n_x):
            paired = paired + rs2[b, i].reshape(group_rows, 2 * units).astype(F32)
        gate, up = paired[:, :units] * factors, paired[:, units:] * factors
        hidden = (silu(gate) * up).astype(BF16)
        hid_all[group_of(0), :, b * units : (b + 1) * units] = hidden.reshape(per_x, tokens, units)
    for i in range(1, n_x):
        remote(
            hid_all.at[group_of(0)],
            hid_all.at[group_of(0)],
            x_send.at[4],
            x_recv.at[4],
            x_peer(i),
        ).start()

    for k in range(EARLY, CHUNKS):
        run_expert(k)

    def go_home(k):
        out = yb[k, 0].astype(F32)
        wait_bytes(yr.at[k, peers_x, :, pl.ds(0, ROWS)], y_recv.at[k])
        for i in range(1, n_x):
            out = out + yr[k, i].astype(F32)
        rb[chunk(k)] = out.astype(BF16)
        for r in range(k * per_chunk, (k + 1) * per_chunk):
            if r:
                remote(
                    rb.at[r, pl.ds(0, ROWS)],
                    ret.at[r, pl.ds(0, ROWS)],
                    pl_send.at[CHUNKS],
                    pl_recv.at[CHUNKS],
                    ep_at(r, -1),
                ).start()
            else:
                ret[0] = rb[0]

    for k in range(EARLY):
        go_home(k)

    wait_bytes(hid_all.at[pl.ds(0, n_yc - per_x)], x_recv.at[4])

    wait_bytes(wd.at[peers_z], wz_recv.at[0])
    dense_part = dot(
        hid_all[...].reshape(n_yc * tokens, all_units), wd[...].reshape(all_units, quarter)
    )
    db[...] = dense_part.reshape(n_yc, tokens, quarter).astype(BF16)
    for i in range(1, n_yc):
        remote(
            db.at[lax.rem(yc + i, n_yc)], dr.at[i], yc_send.at[2], yc_recv.at[2], yc_peer(i)
        ).start()

    for k in range(EARLY, CHUNKS):
        go_home(k)

    dense = db[pl.ds(yc, 1)][0].astype(F32)
    wait_bytes(dr.at[peers_yc], yc_recv.at[2])
    for i in range(1, n_yc):
        dense = dense + dr[i].astype(F32)

    wait_bytes(ret.at[pl.ds(1, n_ep - 1), pl.ds(0, ROWS)], pl_recv.at[CHUNKS])

    back = ret[...].reshape(n_ep * PAD, quarter)
    routed = turned_dot(comb_hi_ref[...], back) + turned_dot(comb_lo_ref[...], back)
    middle_own = mid[pl.ds(x, 1)][0].astype(F32)
    out_ref[...] = (middle_own + branch * dense + routed).astype(BF16)

    for p in range(2):
        wait_bytes(part.at[peers_x, rows_of(p)], x_send.at[p])
        wait_bytes(mid.at[peers_x, rows_of(p)], x_send.at[2 + p])
        wait_bytes(mid_all.at[peers_yc, rows_of(p)], yc_send.at[p])
    wait_bytes(hid_all.at[pl.ds(0, n_yc - per_x)], x_send.at[4])
    for b in range(n_z):
        wait_bytes(rs2.at[b, peers_x], r_send.at[b])
    for k in range(CHUNKS):
        wait_bytes(yb.at[k, peers_x, :, pl.ds(0, ROWS)], y_send.at[k])
    wait_bytes(wgu.at[peers_z], wz_send.at[0])
    wait_bytes(wd.at[peers_z], wz_send.at[1])
    wait_bytes(db.at[peers_yc], yc_send.at[2])
    wait_bytes(fac.at[peers_yc], yc_send.at[3])
    for k in range(CHUNKS):
        wait_bytes(snd.at[others(k), pl.ds(0, ROWS)], pl_send.at[k])
    wait_bytes(rb.at[pl.ds(1, n_ep - 1), pl.ds(0, ROWS)], pl_send.at[CHUNKS])


def emit_kernel(mixed_ref, state_ref, mixed_hbm, state_hbm, sem):
    step = state_ref.shape[0] // 4
    copies = [pltpu.make_async_copy(mixed_ref, mixed_hbm, sem.at[0])]
    for i in range(4):
        rows = pl.ds(i * step, step)
        copies.append(
            pltpu.make_async_copy(state_ref.at[rows], state_hbm.at[rows], sem.at[1 + i])
        )
    for copy in copies:
        copy.start()
    for copy in copies:
        copy.wait()


def emit(mixed, state):
    vmem = pl.BlockSpec(memory_space=pltpu.VMEM)
    hbm = pl.BlockSpec(memory_space=pltpu.HBM)
    return pl.pallas_call(
        emit_kernel,
        name="emit",
        out_shape=(
            jax.ShapeDtypeStruct(mixed.shape, mixed.dtype),
            jax.ShapeDtypeStruct(state.shape, state.dtype),
        ),
        in_specs=[vmem, vmem],
        out_specs=(hbm, hbm),
        scratch_shapes=[pltpu.SemaphoreType.DMA((5,))],
        compiler_params=pltpu.CompilerParams(vmem_limit_bytes=16 << 20),
    )(mixed, state)


def layer(sizes, small, weights, pw, state, expert, dense):
    n_ep, n_x, n_z = sizes
    n_yc = n_ep // n_z
    tokens, width = small[2].shape
    key_dim, value_dim = state.shape[1:]
    eg, dg = expert[0], dense[0]
    quarter, units = width // n_x, dg.shape[1]
    all_units = n_z * units
    flat = n_ep * PAD
    vmem = pl.BlockSpec(memory_space=pltpu.VMEM)
    hbm = pl.BlockSpec(memory_space=pltpu.HBM)
    dma = pltpu.SemaphoreType.DMA
    operands = (*small, *weights, pw, state, *expert, *dense)
    return pl.pallas_call(
        functools.partial(layer_kernel, sizes),
        name="layer",
        out_shape=(
            jax.ShapeDtypeStruct((tokens, quarter), BF16),
            jax.ShapeDtypeStruct(state.shape, F32),
        ),
        in_specs=[hbm] * len(operands),
        out_specs=(vmem, vmem),
        scratch_shapes=[pltpu.VMEM(a.shape, a.dtype) for a in (*small, *weights, pw)]
        + [
            pltpu.VMEM((tokens, key_dim), F32),
            pltpu.VMEM((tokens, key_dim), F32),
            pltpu.VMEM((tokens, value_dim), F32),
            pltpu.VMEM((tokens, key_dim), F32),
            pltpu.VMEM((tokens, value_dim), F32),
            pltpu.VMEM((tokens, value_dim), F32),
            pltpu.VMEM((n_x, tokens, quarter), BF16),
            pltpu.VMEM((flat, tokens), BF16),
            pltpu.VMEM((flat, tokens), BF16),
            pltpu.VMEM((flat, tokens), BF16),
        ]
        + [pltpu.VMEM(a.shape, a.dtype) for a in expert]
        + [
            pltpu.VMEM((n_z, 2, quarter, units), BF16),
            pltpu.VMEM((n_z, units, quarter), BF16),
            pltpu.VMEM((n_x, tokens, quarter), BF16),
            pltpu.VMEM((n_x, tokens, quarter), BF16),
            pltpu.VMEM((n_ep, PAD, width), BF16),
            pltpu.VMEM((n_ep, PAD, width), BF16),
            pltpu.VMEM((n_yc, tokens, quarter), BF16),
            pltpu.VMEM((tokens, width), BF16),
            pltpu.VMEM((n_yc, 8, 128), F32),
            pltpu.VMEM((n_z, n_yc, tokens, 2 * units), BF16),
            pltpu.VMEM((n_z, n_x, n_yc // n_x, tokens, 2 * units), BF16),
            pltpu.VMEM((n_yc, tokens, all_units), BF16),
            pltpu.VMEM((n_yc, tokens, quarter), BF16),
            pltpu.VMEM((n_yc, tokens, quarter), BF16),
            pltpu.VMEM((CHUNKS, n_x, n_ep // CHUNKS, PAD, quarter), BF16),
            pltpu.VMEM((CHUNKS, n_x, n_ep // CHUNKS, PAD, quarter), BF16),
            pltpu.VMEM((n_ep, PAD, quarter), BF16),
            pltpu.VMEM((n_ep, PAD, quarter), BF16),
            dma((14,)),
            dma((tokens // 8,)),
            dma((6,)),
            dma((2,)),
            dma((n_z,)),
            dma((5,)),
            dma((5,)),
            dma((n_z,)),
            dma((n_z,)),
            dma((CHUNKS,)),
            dma((CHUNKS,)),
            dma((4,)),
            dma((4,)),
            dma((CHUNKS + 1,)),
            dma((CHUNKS + 1,)),
        ],
        compiler_params=pltpu.CompilerParams(
            collective_id=0, has_side_effects=True, vmem_limit_bytes=40 << 20
        ),
    )(*in_hbm(*operands))


def body(
    sizes,
    hidden_in,
    carried_state,
    input_gain,
    query_weight,
    key_weight,
    value_weight,
    outgate_weight,
    decay_weight,
    decay_shift,
    head_gain,
    output_weight,
    channel_gain,
    branch_gate,
    routes,
    route_weights,
    expert_gate,
    expert_up,
    expert_down,
    dense_gate,
    dense_up,
    dense_down,
):
    mixed, new_state = layer(
        sizes,
        (
            routes.T,
            route_weights.T,
            hidden_in,
            input_gain,
            decay_shift,
            head_gain,
            channel_gain,
            branch_gate,
        ),
        (query_weight, key_weight, value_weight, outgate_weight, decay_weight),
        output_weight,
        carried_state[:, 0],
        (expert_gate[0], expert_up[0], expert_down[0]),
        (dense_gate, dense_up, dense_down),
    )
    mixed, new_state = emit(mixed, new_state)
    return (mixed, new_state[:, None])


def solution(mesh):
    in_specs = (
        P("ep", None),
        P("ep", "tp", None, None),
        P(),
        P(None, "tp"),
        P(None, "tp"),
        P(None, "tp"),
        P(None, "tp"),
        P(None, "tp"),
        P("ep", "tp"),
        P("tp", None),
        P("tp", None),
        P(),
        P(),
        P("ep", None),
        P("ep", None),
        P("ep", None, "tp"),
        P("ep", None, "tp"),
        P("ep", "tp", None),
        P("tp", "ep"),
        P("tp", "ep"),
        P("ep", "tp"),
    )
    out_specs = (P("ep", "tp"), P("ep", "tp", None, None))
    n_ep = mesh.shape["ep"]
    sizes = (n_ep, mesh.shape["tp"], min(Z_SIZE, n_ep // 2))
    return jax.shard_map(
        functools.partial(body, sizes),
        mesh=mesh,
        in_specs=in_specs,
        out_specs=out_specs,
        check_vma=False,
    )
```
